32 devices in a mesh: sp: 4 (over y, core), tp: 8 (over z, x).
Axes of the slice: x: 2, y: 2, z: 4, core: 2. Of those that a mesh axis runs over, the one named last changes fastest.
Arguments:
- latent: bfloat16 [960, 2048], P(('sp', 'tp')), may hold values from -40 to 40
- context: bfloat16 [768, 2048], P('sp'), may hold values from -6 to 6
- cond_latent: float32 [2048], P('sp'), may hold values from -6 to 6
- cond_context: float32 [2048], P('sp'), may hold values from -6 to 6
- mod_weight: bfloat16 [2048, 6144], P('sp', 'tp'), may hold values from -0.125 to 0.125
- w_query: bfloat16 [2048, 1024], P(None, 'tp'), may hold values from -5 to 5
- w_key: bfloat16 [2048, 1024], P(None, 'tp'), may hold values from -5 to 5
- w_value: bfloat16 [2048, 1024], P(None, 'tp'), may hold values from -0.125 to 0.125
- w_out: bfloat16 [1024, 2048], P('tp'), may hold values from -0.1875 to 0.1875
- head_lambda: float32 [8], P('tp'), may hold values from 0.3 to 0.8
Outputs:
- mixed_latent: bfloat16 [960, 2048], P(('sp', 'tp'))
The draws below stay inside these ranges and needn't reach their ends.
All inputs are finite; a program needn't handle non-finite values.
Results may differ from the reference program's by a relative error of at most 0.011.
Values may be sent and summed in bfloat16 or wider, within the bound.
No kernel may reach another device: no remote copies, remote signals or barrier semaphores. Data moves between devices by JAX's collectives and lax.ppermute only.
A program may use at most 64 MiB of HBM per device.

```python
import jax
import jax.numpy as jnp
from jax import lax

D = 2048
QK_DIM = 64
VAL_DIM = 128
HEADS = 8
GRID_W = 64
CTX = 768
TOKENS = 960


def draw_w_query(key, part):
    projection = jax.random.truncated_normal(jax.random.fold_in(key, 21), -4.0, 4.0, (D, HEADS * 2 * QK_DIM), jnp.float32) * D ** (-0.5)
    return projection.astype(jnp.bfloat16)


def draw_w_key(key, part):
    projection = jax.random.truncated_normal(jax.random.fold_in(key, 22), -4.0, 4.0, (D, HEADS * 2 * QK_DIM), jnp.float32) * D ** (-0.5)
    return projection.astype(jnp.bfloat16)


def draw_latent(key, part):
    filled = jax.random.truncated_normal(jax.random.fold_in(key, 31), -4.0, 4.0, (TOKENS, D), jnp.float32)
    return filled.astype(jnp.bfloat16)


def level_of(rng, dims, shards, low, high):
    gain, own = 1.0, jax.random.fold_in(rng, 6)
    for position, blocks in shards:
        heights = jnp.exp(jax.random.uniform(jax.random.fold_in(own, position), (blocks,), jnp.float32, low / len(shards), high / len(shards)))
        gain = gain * jnp.repeat(heights, dims[position] // blocks).reshape([-1 if axis == position else 1 for axis in range(len(dims))])
    return gain


def centred(key, dims, spread, reach, shards=(), held_as=jnp.bfloat16):
    gain = level_of(key, dims, shards, -0.22, 0.18) if shards else 1.0
    values = jax.random.normal(key, dims, jnp.float32) * spread * gain
    return jnp.minimum(jnp.maximum(values, -reach), reach).astype(held_as)


def setup_inputs(seed: int = 0) -> dict:
    seeds = jax.random.split(jax.random.key(seed), 11)
    latent = draw_latent(jax.random.fold_in(seeds[10], 71), 0)
    context = centred(seeds[1], (CTX, D), 1.0, 6.0, ((0, 4),))
    cond_latent = centred(seeds[2], (D,), 1.0, 6.0, ((0, 4),), jnp.float32)
    cond_context = centred(seeds[3], (D,), 1.0, 6.0, ((0, 4),), jnp.float32)
    mod_weight = centred(seeds[4], (D, 3 * D), D ** -0.5, 0.125, ((0, 4), (1, 8)))
    w_query = draw_w_query(jax.random.fold_in(seeds[10], 71), 0)
    w_key = draw_w_key(jax.random.fold_in(seeds[10], 71), 0)
    w_value = centred(seeds[7], (D, HEADS * VAL_DIM), D ** -0.5, 0.125, ((1, 8),))
    w_out = centred(seeds[8], (HEADS * VAL_DIM, D), (HEADS * VAL_DIM) ** -0.5, 0.1875, ((0, 8),))
    head_lambda = jnp.clip(0.3 + 0.5 * jax.random.uniform(seeds[9], (HEADS,), jnp.float32) ** level_of(seeds[9], (HEADS,), ((0, 8),), -0.2, 0.2), 0.3, 0.8)
    return dict(latent=latent, context=context, cond_latent=cond_latent, cond_context=cond_context, mod_weight=mod_weight, w_query=w_query, w_key=w_key, w_value=w_value, w_out=w_out, head_lambda=head_lambda)


NORM_EPS = 0.01
HEAD_EPS = 0.001
THETA = 10000.0

def modulate_rows(rows, shift, scale):
    values = rows.astype(jnp.float32)
    normed = values * lax.rsqrt(lax.optimization_barrier(jnp.mean(values * values, axis=-1, keepdims=True)) + NORM_EPS)
    return (normed * (1.0 + scale) + shift).astype(jnp.bfloat16)

def rotary_tables(positions):
    quarter = QK_DIM // 4
    inverse = THETA ** (-jnp.arange(quarter, dtype=jnp.float32) / quarter)
    grid_row = (positions // GRID_W).astype(jnp.float32)
    grid_column = (positions % GRID_W).astype(jnp.float32)
    by_row = grid_row[:, None] * inverse[None, :]
    by_column = grid_column[:, None] * inverse[None, :]
    angle = jnp.concatenate([by_row, by_row, by_column, by_column], axis=-1)
    return (jnp.cos(angle), jnp.sin(angle))

def rotate(product, cosine, sine):
    number = product.shape[0]
    quarter = QK_DIM // 4
    half = QK_DIM // 2
    shaped = product.reshape(number, -1, QK_DIM)
    first = shaped[..., :half]
    second = shaped[..., half:]
    turned = jnp.concatenate([-first[..., quarter:], first[..., :quarter], -second[..., quarter:], second[..., :quarter]], axis=-1)
    result = shaped * cosine[:, None, :] + turned * sine[:, None, :]
    return result.reshape(number, -1).astype(jnp.bfloat16)

def one_head(inputs):
    queries, keys, values, factor = inputs
    scores = jnp.einsum('qmd,kmd->mqk', queries.astype(jnp.float32), keys.astype(jnp.float32)) * QK_DIM ** (-0.5)
    highest = lax.optimization_barrier(jnp.max(scores, axis=-1, keepdims=True))
    weights = jnp.exp(scores - highest)
    totals = lax.optimization_barrier(jnp.sum(weights, axis=-1))
    rounded = lax.optimization_barrier(weights.astype(jnp.bfloat16))
    mixed = jnp.einsum('mqk,kd->mqd', rounded.astype(jnp.float32), values.astype(jnp.float32))
    head_out = mixed[0] / totals[0][:, None] - factor * mixed[1] / totals[1][:, None]
    head_out = head_out * lax.rsqrt(lax.optimization_barrier(jnp.mean(head_out * head_out, axis=-1, keepdims=True)) + HEAD_EPS)
    return head_out.astype(jnp.bfloat16)

def reference(latent, context, cond_latent, cond_context, mod_weight, w_query, w_key, w_value, w_out, head_lambda):
    width = latent.shape[1]
    conditioned = jax.nn.silu(jnp.stack([cond_latent, cond_context]).astype(jnp.float32)).astype(jnp.bfloat16)
    modulation = jnp.dot(conditioned, mod_weight, preferred_element_type=jnp.float32)
    normed_latent = modulate_rows(latent, modulation[0, :width], modulation[0, width:2 * width])
    normed_context = modulate_rows(context, modulation[1, :width], modulation[1, width:2 * width])
    cosine, sine = rotary_tables(jnp.arange(TOKENS, dtype=jnp.int32))
    queries = rotate(jnp.dot(normed_latent, w_query, preferred_element_type=jnp.float32), cosine, sine)
    latent_keys = rotate(jnp.dot(normed_latent, w_key, preferred_element_type=jnp.float32), cosine, sine)
    latent_values = jnp.dot(normed_latent, w_value, preferred_element_type=jnp.float32).astype(jnp.bfloat16)
    context_keys = jnp.dot(normed_context, w_key, preferred_element_type=jnp.float32).astype(jnp.bfloat16)
    context_values = jnp.dot(normed_context, w_value, preferred_element_type=jnp.float32).astype(jnp.bfloat16)
    keys = jnp.concatenate([latent_keys, context_keys], axis=0)
    values = jnp.concatenate([latent_values, context_values], axis=0)
    heads = head_lambda.shape[0]
    key_count = keys.shape[0]
    query_heads = jnp.transpose(queries.reshape(TOKENS, heads, 2, QK_DIM), (1, 0, 2, 3))
    key_heads = jnp.transpose(keys.reshape(key_count, heads, 2, QK_DIM), (1, 0, 2, 3))
    value_heads = jnp.transpose(values.reshape(key_count, heads, VAL_DIM), (1, 0, 2))
    attended = lax.map(one_head, (query_heads, key_heads, value_heads, head_lambda.astype(jnp.float32)))
    attended = jnp.transpose(attended, (1, 0, 2)).reshape(TOKENS, heads * VAL_DIM)
    projected = jnp.dot(attended, w_out, preferred_element_type=jnp.float32)
    branch = projected * lax.rsqrt(lax.optimization_barrier(jnp.mean(projected * projected, axis=-1, keepdims=True)) + NORM_EPS)
    return (latent.astype(jnp.float32) + modulation[0, 2 * width:] * branch).astype(jnp.bfloat16)
```

```python
import jax
import jax.numpy as jnp
from jax import lax
from jax.sharding import PartitionSpec as P

QK_DIM = 64
VAL_DIM = 128
GRID_W = 64


NORM_EPS = 0.01
HEAD_EPS = 0.001
THETA = 10000.0


def modulate_rows(rows, shift, scale):
    values = rows.astype(jnp.float32)
    normed = values * lax.rsqrt(jnp.mean(values * values, axis=-1, keepdims=True) + NORM_EPS)
    return (normed * (1.0 + scale) + shift).astype(jnp.bfloat16)


def rotary_tables(positions):
    quarter = QK_DIM // 4
    inverse = THETA ** (-jnp.arange(quarter, dtype=jnp.float32) / quarter)
    grid_row = (positions // GRID_W).astype(jnp.float32)
    grid_column = (positions % GRID_W).astype(jnp.float32)
    by_row = grid_row[:, None] * inverse[None, :]
    by_column = grid_column[:, None] * inverse[None, :]
    angle = jnp.concatenate([by_row, by_row, by_column, by_column], axis=-1)
    return (jnp.cos(angle), jnp.sin(angle))


def rotate(product, cosine, sine):
    number = product.shape[0]
    quarter = QK_DIM // 4
    half = QK_DIM // 2
    shaped = product.reshape(number, -1, QK_DIM)
    first = shaped[..., :half]
    second = shaped[..., half:]
    turned = jnp.concatenate(
        [
            -first[..., quarter:],
            first[..., :quarter],
            -second[..., quarter:],
            second[..., :quarter],
        ],
        axis=-1,
    )
    result = shaped * cosine[:, None, :] + turned * sine[:, None, :]
    return result.reshape(number, -1).astype(jnp.bfloat16)


def shifted(value, axis, step):
    size = lax.axis_size(axis)
    return lax.ppermute(value, axis, [(i, (i + step) % size) for i in range(size)])


def attend_piece(state, piece, queries):
    highest, totals, carried = state
    keys, values = piece
    number = keys.shape[0]
    heads = queries.shape[1]
    key_heads = keys.reshape(number, heads, 2, QK_DIM)
    value_heads = values.reshape(number, heads, VAL_DIM)
    scores = jnp.einsum(
        "qhmd,khmd->hmqk", queries, key_heads, preferred_element_type=jnp.float32
    ) * QK_DIM ** (-0.5)
    new_highest = jnp.maximum(highest, jnp.max(scores, axis=-1))
    weights = jnp.exp(scores - new_highest[..., None])
    totals = jnp.sum(weights, axis=-1)
    mixed = jnp.einsum(
        "hmqk,khd->hmqd",
        weights.astype(jnp.bfloat16),
        value_heads,
        preferred_element_type=jnp.float32,
    )
    carried = mixed
    return (new_highest, totals, carried)


def shards(
    latent,
    context,
    cond_latent,
    cond_context,
    mod_weight,
    w_query,
    w_key,
    w_value,
    w_out,
    head_lambda,
):
    width = latent.shape[1]
    heads = head_lambda.shape[0]
    conditioned = jax.nn.silu(jnp.stack([cond_latent, cond_context])).astype(jnp.bfloat16)
    partial_mod = jnp.dot(conditioned, mod_weight, preferred_element_type=jnp.float32)
    rows, ranks = lax.axis_size("sp"), lax.axis_size("tp")
    copies = jnp.broadcast_to(partial_mod, (rows * ranks,) + partial_mod.shape)
    pieces = lax.all_to_all(copies, ("sp", "tp"), 0, 0)
    pieces = pieces.reshape((rows, ranks) + partial_mod.shape).sum(axis=0)
    modulation = jnp.transpose(pieces, (1, 0, 2)).reshape(2, -1)
    shift_context = modulation[1, :width]
    scale_context = modulation[1, width : 2 * width]
    gate_latent = modulation[0, 2 * width :]
    group_rows = latent.shape[0] * lax.axis_size("tp")
    offset = lax.axis_index("sp") * group_rows
    number = latent.shape[0]
    raw = jnp.concatenate([latent] + [shifted(latent, "tp", k) for k in range(1, ranks)], axis=0)
    piece = modulate_rows(raw, modulation[0, :width], modulation[0, width : 2 * width])
    owner = (lax.axis_index("tp") - jnp.arange(ranks, dtype=jnp.int32)) % ranks
    positions = offset + owner[:, None] * number + jnp.arange(number, dtype=jnp.int32)
    positions = positions.reshape(-1)
    cosine, sine = rotary_tables(positions)
    query_part = rotate(jnp.dot(piece, w_query, preferred_element_type=jnp.float32), cosine, sine)
    key_part = rotate(jnp.dot(piece, w_key, preferred_element_type=jnp.float32), cosine, sine)
    value_part = jnp.dot(piece, w_value, preferred_element_type=jnp.float32).astype(jnp.bfloat16)
    projected = jnp.concatenate([query_part, key_part, value_part], axis=1)
    key_columns = heads * 2 * QK_DIM
    queries = projected[:, :key_columns].reshape(group_rows, heads, 2, QK_DIM)
    keys = projected[:, key_columns : 2 * key_columns]
    values = projected[:, 2 * key_columns :]
    initial = (
        jnp.full((heads, 2, group_rows), -1e30, jnp.float32),
        jnp.zeros((heads, 2, group_rows), jnp.float32),
        jnp.zeros((heads, 2, group_rows, VAL_DIM), jnp.float32),
    )
    own_context = modulate_rows(context, shift_context, scale_context)
    context_keys = jnp.dot(own_context, w_key, preferred_element_type=jnp.float32).astype(
        jnp.bfloat16
    )
    context_values = jnp.dot(own_context, w_value, preferred_element_type=jnp.float32).astype(
        jnp.bfloat16
    )
    joined_keys = jnp.concatenate([keys, context_keys], axis=0)
    joined_values = jnp.concatenate([values, context_values], axis=0)
    state = attend_piece(
        initial,
        (
            lax.all_gather(joined_keys, "sp", axis=0, tiled=True),
            lax.all_gather(joined_values, "sp", axis=0, tiled=True),
        ),
        queries,
    )
    highest, totals, carried = state
    factor = head_lambda[:, None, None]
    head_out = (
        carried[:, 0] / totals[:, 0][..., None] - factor * carried[:, 1] / totals[:, 1][..., None]
    )
    head_out = head_out * lax.rsqrt(
        jnp.mean(head_out * head_out, axis=-1, keepdims=True) + HEAD_EPS
    )
    attended = (
        jnp.transpose(head_out, (1, 0, 2)).reshape(group_rows, heads * VAL_DIM).astype(jnp.bfloat16)
    )
    partial = jnp.dot(attended, w_out, preferred_element_type=jnp.float32)
    partial = partial.astype(jnp.bfloat16).reshape(ranks, number, -1)
    branch = partial[0].astype(jnp.float32)
    for k in range(1, ranks):
        branch = branch + shifted(partial[k], "tp", -k).astype(jnp.float32)
    branch = branch * lax.rsqrt(jnp.mean(branch * branch, axis=-1, keepdims=True) + NORM_EPS)
    return (latent.astype(jnp.float32) + gate_latent * branch).astype(jnp.bfloat16)


def solution(mesh):
    placed = (
        P(("sp", "tp"), None),
        P("sp", None),
        P("sp"),
        P("sp"),
        P("sp", "tp"),
        P(None, "tp"),
        P(None, "tp"),
        P(None, "tp"),
        P("tp", None),
        P("tp"),
    )
    return jax.shard_map(
        shards, mesh=mesh, in_specs=placed, out_specs=P(("sp", "tp"), None), check_vma=False
    )
```

```python
import functools

import jax
import jax.numpy as jnp
from jax import lax
from jax.experimental import pallas as pl
from jax.experimental.pallas import tpu as pltpu
from jax.sharding import PartitionSpec as P

QK_DIM = 64
VAL_DIM = 128
GRID_W = 64

NORM_EPS = 0.01
HEAD_EPS = 0.001
THETA = 10000.0

F32 = jnp.float32
BF16 = jnp.bfloat16
VMEM = pl.BlockSpec(memory_space=pltpu.VMEM)
SMEM = pl.BlockSpec(memory_space=pltpu.SMEM)


def ahead(i, k, n):
    return i ^ k if n & (n - 1) == 0 else (i + k) % n


def behind(i, k, n):
    return i ^ k if n & (n - 1) == 0 else (i - k) % n


def split_of(size):
    inner = max(d for d in range(1, size + 1) if size % d == 0 and d * d <= size)
    return size // inner, inner


def call(body, outs, *args, scratch=(), flops=1000000, in_specs=None):
    return pl.pallas_call(
        body,
        out_shape=outs,
        in_specs=in_specs or [VMEM] * len(args),
        out_specs=jax.tree.map(lambda _: VMEM, outs),
        scratch_shapes=list(scratch),
        compiler_params=pltpu.CompilerParams(vmem_limit_bytes=48 * 1024 * 1024),
        cost_estimate=pl.CostEstimate(flops=flops, bytes_accessed=0, transcendentals=0),
    )(*args)


def sds(shape, dtype):
    return jax.ShapeDtypeStruct(shape, dtype)


def partial_body(latent_ref, context_ref, weight_ref, out_ref):
    def silu(v):
        return v / (1.0 + jnp.exp(-v))

    rows = jnp.concatenate([silu(latent_ref[...]), silu(context_ref[...])], axis=0)
    part = jnp.dot(rows.astype(BF16), weight_ref[...], preferred_element_type=F32)
    for i in range(out_ref.shape[0]):
        out_ref[i] = part


def modulated(values, shift, scale):
    values = values.astype(F32)
    mean = jnp.mean(values * values, axis=-1, keepdims=True)
    return (values * lax.rsqrt(mean + NORM_EPS) * scale + shift).astype(BF16)


def fill_rows(blocks, rows_ref, pad, shift, scale):
    number = blocks[0].shape[0]
    for k, block in enumerate(blocks):
        rows_ref[k * pad : k * pad + number, :] = modulated(block[...], shift, scale)
        if pad > number:
            rows_ref[k * pad + number : (k + 1) * pad, :] = jnp.zeros(
                (pad - number, rows_ref.shape[1]), BF16
            )


def turn(u, cosine, sine):
    lane = lax.broadcasted_iota(jnp.int32, u.shape, 1)
    quarter = QK_DIM // 4
    width = u.shape[1]
    even = (lane // quarter) % 2 == 0
    turned = jnp.where(even, pltpu.roll(u, width - quarter, 1), pltpu.roll(u, quarter, 1))
    return (u * cosine + turned * sine).astype(BF16)


def project_rows(rows, weight_ref, cos_ref, sin_ref, q_ref, kv_ref):
    number = rows.shape[0]
    wide = 2 * QK_DIM
    cosine, sine = cos_ref[...], sin_ref[...]
    u = jnp.dot(rows, weight_ref[...], preferred_element_type=F32)
    q_ref[...] = turn(u[:, :wide], cosine, sine)
    kv_ref[0:number, :wide] = turn(u[:, wide : 2 * wide], cosine, sine)
    kv_ref[0:number, wide:] = u[:, 2 * wide :].astype(BF16)


def first_body(pad, ranks, count, *refs):
    pieces_ref, context_ref, weight_ref, cos_ref, sin_ref = refs[:5]
    blocks = refs[5 : 5 + count]
    mod_ref, q_ref, kv_ref, rows_ref, ctx_ref = refs[5 + count :]
    width = context_ref.shape[1]
    columns = pieces_ref.shape[2]
    groups = pieces_ref.shape[0] // ranks
    for t in range(ranks):
        total = pieces_ref[t]
        for s in range(1, groups):
            total = total + pieces_ref[s * ranks + t]
        mod_ref[:, t * columns : (t + 1) * columns] = total
    mod = mod_ref[...]
    shift, scale = mod[1:2, :width], 1.0 + mod[1:2, width : 2 * width]
    held = context_ref.shape[0]
    step = 16 if held % 16 == 0 else held
    for i in range(0, held, step):
        ctx_ref[i : i + step, :] = modulated(context_ref[i : i + step, :], shift, scale)
    base = count * pad
    wide = 2 * QK_DIM
    kv_ref[base : base + held, :] = jnp.dot(
        ctx_ref[...], weight_ref[:, wide:], preferred_element_type=F32
    ).astype(BF16)
    fill_rows(blocks, rows_ref, pad, mod[0:1, :width], 1.0 + mod[0:1, width : 2 * width])
    project_rows(rows_ref[...], weight_ref, cos_ref, sin_ref, q_ref, kv_ref)


def second_body(pad, count, *refs):
    mod_ref, weight_ref, cos_ref, sin_ref = refs[:4]
    blocks = refs[4 : 4 + count]
    q_ref, kv_ref, rows_ref = refs[4 + count :]
    width = blocks[0].shape[1]
    fill_rows(
        blocks, rows_ref, pad, mod_ref[0:1, :width], 1.0 + mod_ref[0:1, width : 2 * width]
    )
    project_rows(rows_ref[...], weight_ref, cos_ref, sin_ref, q_ref, kv_ref)


def attend_body(number, pad, outer, inner, members, *refs):
    factor_ref = refs[0]
    q_refs = refs[1 : 1 + inner]
    kv_refs = refs[1 + inner : 1 + inner + inner * members]
    out_ref, q_all, k_all, v_all = refs[1 + inner + inner * members :]
    wide = 2 * QK_DIM
    tile = outer * pad
    for j in range(inner):
        q_all[j] = q_refs[j][...] * jnp.asarray(QK_DIM ** (-0.5), BF16)
    row = 0
    for piece in kv_refs:
        k_all[row : row + tile, :] = piece[0:tile, :wide]
        v_all[row : row + tile, :] = piece[0:tile, wide:]
        row += tile
    latents = row
    for piece in kv_refs[:members]:
        held = piece.shape[0] - tile
        k_all[row : row + held, :] = piece[tile : tile + held, :wide]
        v_all[row : row + held, :] = piece[tile : tile + held, wide:]
        row += held
    column = lax.broadcasted_iota(jnp.int32, (1, row), 1)
    valid = (column >= latents) | (column % pad < number)
    bias = jnp.where(valid, 0.0, -1e30)
    lane = lax.broadcasted_iota(jnp.int32, (tile, wide), 1)

    def one(j, carry):
        queries = q_all[j]
        mixed = []
        for m in range(2):
            own = jnp.where((lane // QK_DIM) == m, queries, jnp.zeros_like(queries))
            scores = lax.dot_general(
                own, k_all[...], (((1,), (1,)), ((), ())), preferred_element_type=F32
            )
            scores = scores + bias
            highest = jnp.max(scores, axis=-1, keepdims=True)
            weights = jnp.exp(scores - highest)
            totals = jnp.sum(weights, axis=-1, keepdims=True)
            mix = jnp.dot(weights.astype(BF16), v_all[...], preferred_element_type=F32)
            mixed.append(mix / totals)
        head = mixed[0] - factor_ref[0] * mixed[1]
        head = head * lax.rsqrt(jnp.mean(head * head, axis=-1, keepdims=True) + HEAD_EPS)
        head = head.astype(BF16)
        for k in range(outer):
            out_ref[k, j] = head[k * pad : (k + 1) * pad]
        return carry

    if inner <= 4:
        for j in range(inner):
            one(j, 0)
    else:
        lax.fori_loop(0, inner, one, 0)


def weights_body(share, outer, *refs):
    side_ref, own_ref = refs[:2]
    mine = refs[2 : 1 + outer]
    theirs = refs[1 + outer : 1 + outer + (outer - 1) * (share - 1)]
    out_ref = refs[-1]
    depth = own_ref.shape[0]
    half = depth // share
    out_ref[0:depth, :] = own_ref[...]
    for k in range(1, outer):
        if share == 1:
            out_ref[k * depth : (k + 1) * depth, :] = mine[k - 1][...]
            continue
        start = pl.multiple_of(k * depth + side_ref[0] * half, half)
        other = pl.multiple_of(k * depth + (1 - side_ref[0]) * half, half)
        out_ref[pl.ds(start, half), :] = mine[k - 1][...]
        out_ref[pl.ds(other, half), :] = theirs[k - 1][...]


def partial_out_body(outer, inner, pad, *refs):
    weight_ref = refs[0]
    parts = refs[1 : 1 + outer]
    own_ref = refs[1 + outer]
    others = refs[2 + outer : 1 + outer + inner]
    gathered = refs[-1]
    for k, part in enumerate(parts):
        for j in range(inner):
            gathered[j * pad : (j + 1) * pad, k * VAL_DIM : (k + 1) * VAL_DIM] = part[j]
    total = jnp.dot(gathered[...], weight_ref[...], preferred_element_type=F32)
    own_ref[...] = total[:pad]
    for j in range(1, inner):
        others[j - 1][...] = total[j * pad : (j + 1) * pad].astype(BF16)


def final_body(count, *refs):
    latent_ref, mod_ref, own_ref = refs[:3]
    others = refs[3 : 3 + count]
    out_ref = refs[3 + count]
    number, width = out_ref.shape
    total = own_ref[...]
    for other in others:
        total = total + other[...].astype(F32)
    total = total[:number]
    total = total * lax.rsqrt(jnp.mean(total * total, axis=-1, keepdims=True) + NORM_EPS)
    gate = mod_ref[0:1, 2 * width :]
    out_ref[...] = (latent_ref[...].astype(F32) + gate * total).astype(BF16)


def shards(
    latent,
    context,
    cond_latent,
    cond_context,
    mod_weight,
    w_query,
    w_key,
    w_value,
    w_out,
    head_lambda,
):
    number, width = latent.shape
    groups, ranks = lax.axis_size("sp"), lax.axis_size("tp")
    outer, inner = split_of(ranks)
    pad = -(-number // 16) * 16
    wide = 2 * QK_DIM
    tile = outer * pad
    held = context.shape[0]
    here_sp, here_tp = lax.axis_index("sp"), lax.axis_index("tp")
    here_outer, here_inner = here_tp // inner, here_tp % inner

    def along_outer(value, k, way):
        pairs = [
            (o * inner + i, way(o, k, outer) * inner + i)
            for o in range(outer)
            for i in range(inner)
        ]
        return lax.ppermute(value, "tp", pairs)

    def along_inner(value, j, way):
        pairs = [
            (o * inner + i, o * inner + way(i, j, inner))
            for o in range(outer)
            for i in range(inner)
        ]
        return lax.ppermute(value, "tp", pairs)

    def along_sp(value, s):
        return lax.ppermute(value, "sp", [(i, ahead(i, s, groups)) for i in range(groups)])

    columns = mod_weight.shape[1]
    copies = call(
        partial_body,
        sds((groups * ranks, 2, columns), F32),
        cond_latent.reshape(1, -1),
        cond_context.reshape(1, -1),
        mod_weight,
    )
    pieces = lax.all_to_all(copies, ("sp", "tp"), 0, 0)

    blocks = {(0, 0): latent}
    for k in range(1, outer):
        blocks[k, 0] = along_outer(latent, k, ahead)
    for j in range(1, inner):
        for k in range(outer):
            blocks[k, j] = along_inner(blocks[k, 0], j, ahead)

    weight = jnp.concatenate([w_query, w_key, w_value], axis=1)

    lane = jnp.arange(wide, dtype=jnp.int32)[None, :]
    quarter = QK_DIM // 4
    inverse = THETA ** (-(lane % quarter).astype(F32) / quarter)
    sign = jnp.where((lane // quarter) % 2 == 0, -1.0, 1.0)
    line = jnp.arange(tile, dtype=jnp.int32)[:, None]

    def tables(j):
        owner_outer = behind(here_outer, line // pad, outer)
        owner = owner_outer * inner + behind(here_inner, j, inner)
        position = (here_sp * ranks + owner) * number + line % pad
        place = jnp.where(
            (lane % QK_DIM) < QK_DIM // 2, position // GRID_W, position % GRID_W
        ).astype(F32)
        angle = place * inverse
        return jnp.cos(angle), jnp.sin(angle) * sign

    cosine, sine = tables(0)
    mod, q_first, kv_first = call(
        functools.partial(first_body, pad, ranks, outer),
        (
            sds((2, columns * ranks), F32),
            sds((tile, wide), BF16),
            sds((tile + held, wide + VAL_DIM), BF16),
        ),
        pieces,
        context,
        weight,
        cosine,
        sine,
        *[blocks[k, 0] for k in range(outer)],
        scratch=[pltpu.VMEM((tile, width), BF16), pltpu.VMEM((held, width), BF16)],
    )
    queries, kv = [q_first], [kv_first]
    for j in range(1, inner):
        cosine, sine = tables(j)
        q_next, kv_next = call(
            functools.partial(second_body, pad, outer),
            (sds((tile, wide), BF16), sds((tile, wide + VAL_DIM), BF16)),
            mod,
            weight,
            cosine,
            sine,
            *[blocks[k, j] for k in range(outer)],
            scratch=[pltpu.VMEM((tile, width), BF16)],
        )
        queries.append(q_next)
        kv.append(kv_next)
    pieces_kv = []
    for part in kv:
        pieces_kv.append(part)
        pieces_kv += [along_sp(part, s) for s in range(1, groups)]
    keys = groups * (inner * tile + held)
    attended = call(
        functools.partial(attend_body, number, pad, outer, inner, groups),
        sds((outer, inner, pad, VAL_DIM), BF16),
        head_lambda,
        *queries,
        *pieces_kv,
        scratch=[
            pltpu.VMEM((inner, tile, wide), BF16),
            pltpu.VMEM((keys, wide), BF16),
            pltpu.VMEM((keys, VAL_DIM), BF16),
        ],
        in_specs=[SMEM] + [VMEM] * (inner + inner * groups),
    )
    parts = [attended[0]] + [along_outer(attended[k], k, behind) for k in range(1, outer)]

    share = 2 if groups % 2 == 0 else 1
    depth = w_out.shape[0]
    side = here_sp % share
    half = lax.dynamic_slice(w_out, (side * (depth // share), 0), (depth // share, width))
    half, _ = lax.optimization_barrier((half, blocks[outer - 1, 0]))
    mine = [along_outer(half, k, behind) for k in range(1, outer)]
    theirs = []
    if share > 1:
        swap = [(i, i ^ 1) for i in range(groups)]
        theirs = [lax.ppermute(v, "sp", swap) for v in mine]
    weight_out = call(
        functools.partial(weights_body, share, outer),
        sds((outer * depth, width), BF16),
        side.reshape(1).astype(jnp.int32),
        w_out,
        *mine,
        *theirs,
        in_specs=[SMEM] + [VMEM] * (1 + len(mine) + len(theirs)),
    )
    total = call(
        functools.partial(partial_out_body, outer, inner, pad),
        (sds((pad, width), F32),) + (sds((pad, width), BF16),) * (inner - 1),
        weight_out,
        *parts,
        scratch=[pltpu.VMEM((inner * pad, outer * VAL_DIM), BF16)],
    )
    arrived = [along_inner(total[j], j, behind) for j in range(1, inner)]
    return call(
        functools.partial(final_body, inner - 1),
        sds((number, width), BF16),
        latent,
        mod,
        total[0],
        *arrived,
    )


def solution(mesh):
    placed = (
        P(("sp", "tp"), None),
        P("sp", None),
        P("sp"),
        P("sp"),
        P("sp", "tp"),
        P(None, "tp"),
        P(None, "tp"),
        P(None, "tp"),
        P("tp", None),
        P("tp"),
    )
    return jax.shard_map(
        shards, mesh=mesh, in_specs=placed, out_specs=P(("sp", "tp"), None), check_vma=False
    )
```

```python
import functools

import jax
import jax.numpy as jnp
import numpy as np
from jax import lax
from jax.experimental import pallas as pl
from jax.experimental.pallas import tpu as pltpu
from jax.sharding import PartitionSpec as P

QK_DIM = 64
VAL_DIM = 128
GRID_W = 64

NORM_EPS = 0.01
HEAD_EPS = 0.001
THETA = 10000.0

F32 = jnp.float32
BF16 = jnp.bfloat16
VMEM = pl.BlockSpec(memory_space=pltpu.VMEM)
SMEM = pl.BlockSpec(memory_space=pltpu.SMEM)
HBM = pl.BlockSpec(memory_space=pltpu.HBM)


def ahead(i, k, n):
    return i ^ k if n & (n - 1) == 0 else (i + k) % n


def behind(i, k, n):
    return i ^ k if n & (n - 1) == 0 else (i - k) % n


def split_of(size):
    inner = max(d for d in range(1, size + 1) if size % d == 0 and d * d <= size)
    return size // inner, inner


def size_of(v):
    return int(np.prod(v.shape)) * jnp.dtype(v.dtype).itemsize


def call(body, outs, *args, scratch=(), extra=0, local=False, flops=2000000, in_specs=None):
    held = sum(size_of(v) for v in args) + sum(size_of(v) for v in jax.tree.leaves(outs))
    held += sum(size_of(v) for v in scratch if hasattr(v, "dtype") and v.dtype in (F32, BF16))
    limit = min(60 * 1024 * 1024, held + extra + 6 * 1024 * 1024)
    in_specs = in_specs or [VMEM] * len(args)
    args = [
        pltpu.with_memory_space_constraint(v, pltpu.HBM) if spec is HBM else v
        for v, spec in zip(args, in_specs)
    ]
    if local:
        outs = jax.tree.map(lambda v: pltpu.VMEM(v.shape, v.dtype), outs)
    return pl.pallas_call(
        body,
        out_shape=outs,
        in_specs=in_specs,
        out_specs=jax.tree.map(lambda _: VMEM, outs),
        scratch_shapes=list(scratch),
        compiler_params=pltpu.CompilerParams(vmem_limit_bytes=limit),
        cost_estimate=pl.CostEstimate(flops=flops, bytes_accessed=0, transcendentals=0),
    )(*args)


def sds(shape, dtype):
    return jax.ShapeDtypeStruct(shape, dtype)


def partial_body(latent_hbm, context_hbm, weight_hbm, out_ref, cond_ref, weight_ref, sems):
    moves = [
        pltpu.make_async_copy(weight_hbm, weight_ref, sems.at[0]),
        pltpu.make_async_copy(latent_hbm, cond_ref.at[0:1], sems.at[1]),
        pltpu.make_async_copy(context_hbm, cond_ref.at[1:2], sems.at[2]),
    ]
    for move in moves:
        move.start()
    moves[1].wait()
    moves[2].wait()
    rows = cond_ref[...]
    rows = (rows / (1.0 + jnp.exp(-rows))).astype(BF16)
    moves[0].wait()
    part = jnp.dot(rows, weight_ref[...], preferred_element_type=F32)
    for i in range(out_ref.shape[0]):
        out_ref[i] = part


def table_body(number, pad, ranks, outer, inner, *refs):
    here_ref = refs[0]
    sources, (out_ref, weight_ref, sems) = refs[1:4], refs[4:]
    moves = fetch_weights(sources, weight_ref, sems)
    here = here_ref[0]
    group, rank = lax.div(here, ranks), lax.rem(here, ranks)
    here_outer, here_inner = lax.div(rank, inner), lax.rem(rank, inner)
    lane = lax.broadcasted_iota(jnp.int32, (pad, 2 * QK_DIM), 1)
    line = lax.broadcasted_iota(jnp.int32, (pad, 2 * QK_DIM), 0)
    low = lane < QK_DIM
    by_row = (lane & (QK_DIM - 1)) < QK_DIM // 2
    sign = jnp.where((lane & (QK_DIM // 4)) == 0, -1.0, 1.0)
    phase = jnp.where(low, np.float32(np.pi / 2), np.float32(0))
    shift = GRID_W.bit_length() - 1
    quarter = QK_DIM // 4
    inverse = jnp.ones(lane.shape, F32)
    for i in range(1, quarter):
        inverse = jnp.where((lane & (quarter - 1)) == i, np.float32(THETA ** (-i / quarter)), inverse)

    def owner(i, k, n):
        return i ^ k if n & (n - 1) == 0 else lax.rem(i + (n - k), n)

    for j in range(inner):
        for k in range(outer):
            rank_at = owner(here_outer, k, outer) * inner + owner(here_inner, j, inner)
            position = line + (group * ranks + rank_at) * number
            place = jnp.where(by_row, position >> shift, position & (GRID_W - 1)).astype(F32)
            wave = jnp.sin(place * inverse + phase)
            other = pltpu.roll(wave, QK_DIM, 1)
            out_ref[j, 0, k * pad : (k + 1) * pad, :] = jnp.where(low, wave, other)
            out_ref[j, 1, k * pad : (k + 1) * pad, :] = jnp.where(low, other, wave) * sign
    for move in moves:
        move.wait()


def fetch_weights(sources, weight_ref, sems):
    moves, start = [], 0
    for i, source in enumerate(sources):
        columns = source.shape[1]
        moves.append(
            pltpu.make_async_copy(source, weight_ref.at[:, start : start + columns], sems.at[i])
        )
        moves[-1].start()
        start += columns
    return moves


def modulated(values, shift, scale):
    values = values.astype(F32)
    mean = jnp.mean(values * values, axis=-1, keepdims=True)
    return (values * lax.rsqrt(mean + NORM_EPS) * scale + shift).astype(BF16)


def fill_rows(blocks, rows_ref, pad, shift, scale):
    number = blocks[0].shape[0]
    for k, block in enumerate(blocks):
        rows_ref[k * pad : k * pad + number, :] = modulated(block[...], shift, scale)
        if pad > number:
            rows_ref[k * pad + number : (k + 1) * pad, :] = jnp.zeros(
                (pad - number, rows_ref.shape[1]), BF16
            )


def turn(u, cosine, sine):
    lane = lax.broadcasted_iota(jnp.int32, u.shape, 1)
    quarter = QK_DIM // 4
    width = u.shape[1]
    even = (lane // quarter) % 2 == 0
    turned = jnp.where(even, pltpu.roll(u, width - quarter, 1), pltpu.roll(u, quarter, 1))
    return (u * cosine + turned * sine).astype(BF16)


def project_rows(rows, weight_ref, table_ref, j, q_ref, kv_ref):
    number = rows.shape[0]
    wide = 2 * QK_DIM
    cosine, sine = table_ref[j, 0], table_ref[j, 1]
    u = jnp.dot(rows, weight_ref[...], preferred_element_type=F32)
    q_ref[...] = turn(u[:, :wide], cosine, sine)
    kv_ref[0:number, :wide] = turn(u[:, wide : 2 * wide], cosine, sine)
    kv_ref[0:number, wide:] = u[:, 2 * wide :].astype(BF16)


def first_body(pad, ranks, count, *refs):
    pieces_ref, context_ref, table_ref, weight_ref = refs[:4]
    blocks = refs[4 : 4 + count]
    mod_ref, q_ref, kv_ref, rows_ref, ctx_ref = refs[4 + count :]
    width = context_ref.shape[1]
    columns = pieces_ref.shape[2]
    groups = pieces_ref.shape[0] // ranks
    for t in range(ranks):
        total = pieces_ref[t]
        for s in range(1, groups):
            total = total + pieces_ref[s * ranks + t]
        mod_ref[:, t * columns : (t + 1) * columns] = total
    mod = mod_ref[...]
    shift, scale = mod[1:2, :width], 1.0 + mod[1:2, width : 2 * width]
    held = context_ref.shape[0]
    step = 16 if held % 16 == 0 else held
    for i in range(0, held, step):
        ctx_ref[i : i + step, :] = modulated(context_ref[i : i + step, :], shift, scale)
    fill_rows(blocks, rows_ref, pad, mod[0:1, :width], 1.0 + mod[0:1, width : 2 * width])
    base = count * pad
    wide = 2 * QK_DIM
    kv_ref[base : base + held, :] = jnp.dot(
        ctx_ref[...], weight_ref[:, wide:], preferred_element_type=F32
    ).astype(BF16)
    project_rows(rows_ref[...], weight_ref, table_ref, 0, q_ref, kv_ref)


def second_body(pad, count, j, *refs):
    mod_ref, table_ref, weight_ref = refs[:3]
    blocks = refs[3 : 3 + count]
    q_ref, kv_ref, rows_ref = refs[3 + count :]
    width = blocks[0].shape[1]
    fill_rows(
        blocks, rows_ref, pad, mod_ref[0:1, :width], 1.0 + mod_ref[0:1, width : 2 * width]
    )
    project_rows(rows_ref[...], weight_ref, table_ref, j, q_ref, kv_ref)


def attend_body(number, pad, outer, inner, members, *refs):
    factor_ref = refs[0]
    q_refs = refs[1 : 1 + inner]
    kv_refs = refs[1 + inner : 1 + inner + inner * members]
    out_ref, q_all, k_all, v_all = refs[1 + inner + inner * members :]
    wide = 2 * QK_DIM
    tile = outer * pad
    for j in range(inner):
        q_all[j] = q_refs[j][...] * jnp.asarray(QK_DIM ** (-0.5), BF16)
    row = 0
    for piece in kv_refs:
        k_all[row : row + tile, :] = piece[0:tile, :wide]
        v_all[row : row + tile, :] = piece[0:tile, wide:]
        row += tile
    latents = row
    for piece in kv_refs[:members]:
        held = piece.shape[0] - tile
        k_all[row : row + held, :] = piece[tile : tile + held, :wide]
        v_all[row : row + held, :] = piece[tile : tile + held, wide:]
        row += held
    column = lax.broadcasted_iota(jnp.int32, (1, row), 1)
    valid = (column >= latents) | (column % pad < number)
    bias = jnp.where(valid, 0.0, -1e30)
    lane = lax.broadcasted_iota(jnp.int32, (tile, wide), 1)

    def one(j, carry):
        queries = q_all[j]
        mixed = []
        for m in range(2):
            own = jnp.where((lane // QK_DIM) == m, queries, jnp.zeros_like(queries))
            scores = lax.dot_general(
                own, k_all[...], (((1,), (1,)), ((), ())), preferred_element_type=F32
            )
            scores = scores + bias
            highest = jnp.max(scores, axis=-1, keepdims=True)
            weights = jnp.exp(scores - highest)
            totals = jnp.sum(weights, axis=-1, keepdims=True)
            mix = jnp.dot(weights.astype(BF16), v_all[...], preferred_element_type=F32)
            mixed.append(mix / totals)
        head = mixed[0] - factor_ref[0] * mixed[1]
        head = head * lax.rsqrt(jnp.mean(head * head, axis=-1, keepdims=True) + HEAD_EPS)
        head = head.astype(BF16)
        for k in range(outer):
            out_ref[k, j] = head[k * pad : (k + 1) * pad]
        return carry

    if inner <= 4:
        for j in range(inner):
            one(j, 0)
    else:
        lax.fori_loop(0, inner, one, 0)


def partial_out_body(share, outer, inner, pad, *refs):
    side_ref, weight_ref = refs[:2]
    mine = refs[2 : 1 + outer]
    theirs = refs[1 + outer : 1 + outer + (outer - 1) * (share - 1)]
    rest = refs[1 + outer + (outer - 1) * (share - 1) :]
    parts, own_ref, others = rest[:outer], rest[outer], rest[1 + outer :]
    rows = inner * pad
    half = VAL_DIM // share
    total = jnp.dot(
        parts[0][...].reshape(rows, VAL_DIM), weight_ref[...], preferred_element_type=F32
    )
    for k in range(1, outer):
        part = parts[k][...].reshape(rows, VAL_DIM)
        if share == 1:
            total += jnp.dot(part, mine[k - 1][...], preferred_element_type=F32)
            continue
        first = jnp.broadcast_to(side_ref[0], (rows, half)) == 0
        left, right = part[:, :half], part[:, half:]
        total += jnp.dot(
            jnp.where(first, left, right), mine[k - 1][...], preferred_element_type=F32
        )
        total += jnp.dot(
            jnp.where(first, right, left), theirs[k - 1][...], preferred_element_type=F32
        )
    own_ref[...] = total[:pad]
    for j in range(1, inner):
        others[j - 1][...] = total[j * pad : (j + 1) * pad].astype(BF16)


def final_body(count, *refs):
    latent_ref, mod_ref, own_ref = refs[:3]
    others = refs[3 : 3 + count]
    out_ref = refs[3 + count]
    number, width = out_ref.shape
    total = own_ref[...]
    for other in others:
        total = total + other[...].astype(F32)
    total = total[:number]
    total = total * lax.rsqrt(jnp.mean(total * total, axis=-1, keepdims=True) + NORM_EPS)
    gate = mod_ref[0:1, 2 * width :]
    out_ref[...] = (latent_ref[...].astype(F32) + gate * total).astype(BF16)


def shards(
    latent,
    context,
    cond_latent,
    cond_context,
    mod_weight,
    w_query,
    w_key,
    w_value,
    w_out,
    head_lambda,
):
    number, width = latent.shape
    groups, ranks = lax.axis_size("sp"), lax.axis_size("tp")
    outer, inner = split_of(ranks)
    pad = -(-number // 16) * 16
    wide = 2 * QK_DIM
    tile = outer * pad
    held = context.shape[0]
    here_sp, here_tp = lax.axis_index("sp"), lax.axis_index("tp")

    def along_outer(value, k, way):
        pairs = [
            (o * inner + i, way(o, k, outer) * inner + i)
            for o in range(outer)
            for i in range(inner)
        ]
        return lax.ppermute(value, "tp", pairs)

    def along_inner(value, j, way):
        pairs = [
            (o * inner + i, o * inner + way(i, j, inner))
            for o in range(outer)
            for i in range(inner)
        ]
        return lax.ppermute(value, "tp", pairs)

    def along_sp(value, s):
        return lax.ppermute(value, "sp", [(i, ahead(i, s, groups)) for i in range(groups)])

    columns = mod_weight.shape[1]
    copies = call(
        partial_body,
        sds((groups * ranks, 2, columns), F32),
        cond_latent.reshape(1, -1),
        cond_context.reshape(1, -1),
        mod_weight,
        scratch=[
            pltpu.VMEM((2, cond_latent.shape[0]), F32),
            pltpu.VMEM(mod_weight.shape, BF16),
            pltpu.SemaphoreType.DMA((3,)),
        ],
        in_specs=[HBM] * 3,
        local=True,
    )
    pieces = lax.all_to_all(copies, ("sp", "tp"), 0, 0)

    blocks = {(0, 0): latent}
    for k in range(1, outer):
        blocks[k, 0] = along_outer(latent, k, ahead)
    for j in range(1, inner):
        for k in range(outer):
            blocks[k, j] = along_inner(blocks[k, 0], j, ahead)

    here = (here_sp * ranks + here_tp).astype(jnp.int32).reshape(1)
    joined = wide + wide + VAL_DIM
    table, weight = call(
        functools.partial(table_body, number, pad, ranks, outer, inner),
        (sds((inner, 2, tile, wide), F32), sds((width, joined), BF16)),
        here,
        w_query,
        w_key,
        w_value,
        scratch=[pltpu.SemaphoreType.DMA((3,))],
        in_specs=[SMEM] + [HBM] * 3,
        local=True,
    )
    mod, q_first, kv_first = call(
        functools.partial(first_body, pad, ranks, outer),
        (
            sds((2, columns * ranks), F32),
            sds((tile, wide), BF16),
            sds((tile + held, wide + VAL_DIM), BF16),
        ),
        pieces,
        context,
        table,
        weight,
        *[blocks[k, 0] for k in range(outer)],
        scratch=[pltpu.VMEM((tile, width), BF16), pltpu.VMEM((held, width), BF16)],
    )
    queries, kv = [q_first], [kv_first]
    for j in range(1, inner):
        q_next, kv_next = call(
            functools.partial(second_body, pad, outer, j),
            (sds((tile, wide), BF16), sds((tile, wide + VAL_DIM), BF16)),
            mod,
            table,
            weight,
            *[blocks[k, j] for k in range(outer)],
            scratch=[pltpu.VMEM((tile, width), BF16)],
        )
        queries.append(q_next)
        kv.append(kv_next)
    pieces_kv = []
    for part in kv:
        pieces_kv.append(part)
        for s in range(1, groups):
            pieces_kv.append(along_sp(part, s))
    keys = groups * (inner * tile + held)
    attended = call(
        functools.partial(attend_body, number, pad, outer, inner, groups),
        sds((outer, inner, pad, VAL_DIM), BF16),
        head_lambda,
        *queries,
        *pieces_kv,
        scratch=[
            pltpu.VMEM((inner, tile, wide), BF16),
            pltpu.VMEM((keys, wide), BF16),
            pltpu.VMEM((keys, VAL_DIM), BF16),
        ],
        extra=tile * keys * 12,
        in_specs=[SMEM] + [VMEM] * (inner + inner * groups),
    )
    parts = [attended[0]]
    for k in range(1, outer):
        parts.append(along_outer(attended[k], k, behind))

    share = 2 if groups % 2 == 0 else 1
    depth = w_out.shape[0]
    side = here_sp % share
    half = lax.dynamic_slice(w_out, (side * (depth // share), 0), (depth // share, width))
    swap = [(i, i ^ 1) for i in range(groups)]
    mine, theirs = [], []
    for k in range(1, outer):
        mine.append(along_outer(half, k, behind))
        if share > 1:
            theirs.append(lax.ppermute(mine[-1], "sp", swap))
    total = call(
        functools.partial(partial_out_body, share, outer, inner, pad),
        (sds((pad, width), F32),) + (sds((pad, width), BF16),) * (inner - 1),
        side.reshape(1).astype(jnp.int32),
        w_out,
        *mine,
        *theirs,
        *parts,
        in_specs=[SMEM] + [VMEM] * (1 + len(mine) + len(theirs) + outer),
    )
    arrived = []
    for j in range(1, inner):
        arrived.append(along_inner(total[j], j, behind))
    return call(
        functools.partial(final_body, inner - 1),
        sds((number, width), BF16),
        latent,
        mod,
        total[0],
        *arrived,
    )


def solution(mesh):
    placed = (
        P(("sp", "tp"), None),
        P("sp", None),
        P("sp"),
        P("sp"),
        P("sp", "tp"),
        P(None, "tp"),
        P(None, "tp"),
        P(None, "tp"),
        P("tp", None),
        P("tp"),
    )
    return jax.shard_map(
        shards, mesh=mesh, in_specs=placed, out_specs=P(("sp", "tp"), None), check_vma=False
    )
```

```python
import functools

import jax
import jax.numpy as jnp
import numpy as np
from jax import lax
from jax.experimental import pallas as pl
from jax.experimental.pallas import tpu as pltpu
from jax.sharding import PartitionSpec as P

QK_DIM = 64
VAL_DIM = 128
GRID_W = 64

NORM_EPS = 0.01
HEAD_EPS = 0.001
THETA = 10000.0

F32 = jnp.float32
BF16 = jnp.bfloat16
VMEM = pl.BlockSpec(memory_space=pltpu.VMEM)
SMEM = pl.BlockSpec(memory_space=pltpu.SMEM)
NEAR = pl.BlockSpec(memory_space=pltpu.VMEM)
HBM = pl.BlockSpec(memory_space=pltpu.HBM)


def ahead(i, k, n):
    return i ^ k if n & (n - 1) == 0 else (i + k) % n


def behind(i, k, n):
    return i ^ k if n & (n - 1) == 0 else (i - k) % n


def split_of(size):
    inner = max(d for d in range(1, size + 1) if size % d == 0 and d * d <= size)
    return size // inner, inner


def size_of(v):
    return int(np.prod(v.shape)) * jnp.dtype(v.dtype).itemsize


def call(body, outs, *args, scratch=(), extra=0, local=False, flops=2000000, in_specs=None):
    held = sum(size_of(v) for v in args) + sum(size_of(v) for v in jax.tree.leaves(outs))
    held += sum(size_of(v) for v in scratch if hasattr(v, "dtype") and v.dtype in (F32, BF16))
    limit = min(60 * 1024 * 1024, held + extra + 6 * 1024 * 1024)
    in_specs = in_specs or [VMEM] * len(args)
    args = [
        pltpu.with_memory_space_constraint(v, pltpu.HBM)
        if spec is HBM
        else pltpu.with_memory_space_constraint(v, pltpu.VMEM)
        if spec is NEAR
        else v
        for v, spec in zip(args, in_specs)
    ]
    if local:
        outs = jax.tree.map(lambda v: pltpu.VMEM(v.shape, v.dtype), outs)
    return pl.pallas_call(
        body,
        out_shape=outs,
        in_specs=in_specs,
        out_specs=jax.tree.map(lambda _: VMEM, outs),
        scratch_shapes=list(scratch),
        compiler_params=pltpu.CompilerParams(vmem_limit_bytes=limit),
        cost_estimate=pl.CostEstimate(flops=flops, bytes_accessed=0, transcendentals=0),
    )(*args)


def sds(shape, dtype):
    return jax.ShapeDtypeStruct(shape, dtype)


def partial_body(latent_hbm, context_hbm, weight_hbm, out_ref, cond_ref, weight_ref, sems):
    moves = [
        pltpu.make_async_copy(weight_hbm, weight_ref, sems.at[0]),
        pltpu.make_async_copy(latent_hbm, cond_ref.at[0:1], sems.at[1]),
        pltpu.make_async_copy(context_hbm, cond_ref.at[1:2], sems.at[2]),
    ]
    for move in moves:
        move.start()
    moves[1].wait()
    moves[2].wait()
    rows = cond_ref[...]
    rows = (rows / (1.0 + jnp.exp(-rows))).astype(BF16)
    moves[0].wait()
    part = jnp.dot(rows, weight_ref[...], preferred_element_type=F32)
    for i in range(out_ref.shape[0]):
        out_ref[i] = part


def table_body(number, pad, ranks, outer, inner, *refs):
    here_ref = refs[0]
    sources, (out_ref, weight_ref, sems) = refs[1:4], refs[4:]
    moves = fetch_weights(sources, weight_ref, sems)
    here = here_ref[0]
    group, rank = lax.div(here, ranks), lax.rem(here, ranks)
    here_outer, here_inner = lax.div(rank, inner), lax.rem(rank, inner)
    lane = lax.broadcasted_iota(jnp.int32, (pad, 2 * QK_DIM), 1)
    line = lax.broadcasted_iota(jnp.int32, (pad, 2 * QK_DIM), 0)
    low = lane < QK_DIM
    by_row = (lane & (QK_DIM - 1)) < QK_DIM // 2
    sign = jnp.where((lane & (QK_DIM // 4)) == 0, -1.0, 1.0)
    phase = jnp.where(low, np.float32(np.pi / 2), np.float32(0))
    shift = GRID_W.bit_length() - 1
    quarter = QK_DIM // 4
    inverse = jnp.ones(lane.shape, F32)
    for i in range(1, quarter):
        inverse = jnp.where((lane & (quarter - 1)) == i, np.float32(THETA ** (-i / quarter)), inverse)

    def owner(i, k, n):
        return i ^ k if n & (n - 1) == 0 else lax.rem(i + (n - k), n)

    for j in range(inner):
        for k in range(outer):
            rank_at = owner(here_outer, k, outer) * inner + owner(here_inner, j, inner)
            position = line + (group * ranks + rank_at) * number
            place = jnp.where(by_row, position >> shift, position & (GRID_W - 1)).astype(F32)
            wave = jnp.sin(place * inverse + phase)
            other = pltpu.roll(wave, QK_DIM, 1)
            out_ref[j, 0, k * pad : (k + 1) * pad, :] = jnp.where(low, wave, other)
            out_ref[j, 1, k * pad : (k + 1) * pad, :] = jnp.where(low, other, wave) * sign
    for move in moves:
        move.wait()


def fetch_weights(sources, weight_ref, sems):
    moves, start = [], 0
    for i, source in enumerate(sources):
        columns = source.shape[1]
        moves.append(
            pltpu.make_async_copy(source, weight_ref.at[:, start : start + columns], sems.at[i])
        )
        moves[-1].start()
        start += columns
    return moves


def modulated(values, shift, scale):
    values = values.astype(F32)
    mean = jnp.mean(values * values, axis=-1, keepdims=True)
    return (values * lax.rsqrt(mean + NORM_EPS) * scale + shift).astype(BF16)


def fill_rows(blocks, rows_ref, pad, shift, scale):
    number = blocks[0].shape[0]
    for k, block in enumerate(blocks):
        rows_ref[k * pad : k * pad + number, :] = modulated(block[...], shift, scale)
        if pad > number:
            rows_ref[k * pad + number : (k + 1) * pad, :] = jnp.zeros(
                (pad - number, rows_ref.shape[1]), BF16
            )


def turn(u, cosine, sine):
    lane = lax.broadcasted_iota(jnp.int32, u.shape, 1)
    quarter = QK_DIM // 4
    width = u.shape[1]
    even = (lane // quarter) % 2 == 0
    turned = jnp.where(even, pltpu.roll(u, width - quarter, 1), pltpu.roll(u, quarter, 1))
    return (u * cosine + turned * sine).astype(BF16)


def project_rows(rows, weight_ref, table_ref, j, q_ref, kv_ref):
    number = rows.shape[0]
    wide = 2 * QK_DIM
    cosine, sine = table_ref[j, 0], table_ref[j, 1]
    u = jnp.dot(rows, weight_ref[...], preferred_element_type=F32)
    q_ref[...] = turn(u[:, :wide], cosine, sine)
    kv_ref[0:number, :wide] = turn(u[:, wide : 2 * wide], cosine, sine)
    kv_ref[0:number, wide:] = u[:, 2 * wide :].astype(BF16)


def first_body(pad, ranks, count, *refs):
    pieces_ref, context_ref, table_ref, weight_ref = refs[:4]
    blocks = refs[4 : 4 + count]
    mod_ref, q_ref, kv_ref, rows_ref, ctx_ref = refs[4 + count :]
    width = context_ref.shape[1]
    columns = pieces_ref.shape[2]
    groups = pieces_ref.shape[0] // ranks
    for t in range(ranks):
        total = pieces_ref[t]
        for s in range(1, groups):
            total = total + pieces_ref[s * ranks + t]
        mod_ref[:, t * columns : (t + 1) * columns] = total
    mod = mod_ref[...]
    shift, scale = mod[1:2, :width], 1.0 + mod[1:2, width : 2 * width]
    held = context_ref.shape[0]
    step = 16 if held % 16 == 0 else held
    for i in range(0, held, step):
        ctx_ref[i : i + step, :] = modulated(context_ref[i : i + step, :], shift, scale)
    fill_rows(blocks, rows_ref, pad, mod[0:1, :width], 1.0 + mod[0:1, width : 2 * width])
    base = count * pad
    wide = 2 * QK_DIM
    kv_ref[base : base + held, :] = jnp.dot(
        ctx_ref[...], weight_ref[:, wide:], preferred_element_type=F32
    ).astype(BF16)
    project_rows(rows_ref[...], weight_ref, table_ref, 0, q_ref, kv_ref)


def second_body(pad, count, j, *refs):
    mod_ref, table_ref, weight_ref = refs[:3]
    blocks = refs[3 : 3 + count]
    q_ref, kv_ref, rows_ref = refs[3 + count :]
    width = blocks[0].shape[1]
    fill_rows(
        blocks, rows_ref, pad, mod_ref[0:1, :width], 1.0 + mod_ref[0:1, width : 2 * width]
    )
    project_rows(rows_ref[...], weight_ref, table_ref, j, q_ref, kv_ref)


def gather_pieces(pieces, k_all, v_all, number, pad):
    wide = 2 * QK_DIM
    row = 0
    for piece, rows in pieces:
        k_all[row : row + rows, :] = piece[0:rows, :wide]
        v_all[row : row + rows, :] = piece[0:rows, wide:]
        row += rows
    latents = row
    for piece, rows in pieces:
        held = piece.shape[0] - rows
        if held:
            k_all[row : row + held, :] = piece[rows : rows + held, :wide]
            v_all[row : row + held, :] = piece[rows : rows + held, wide:]
            row += held
    column = lax.broadcasted_iota(jnp.int32, (1, row), 1)
    valid = (column >= latents) | (column % pad < number)
    return jnp.where(valid, 0.0, -1e30)


def score(q_all, j, m, k_all, bias):
    queries = q_all[j] * jnp.asarray(QK_DIM ** (-0.5), BF16)
    lane = lax.broadcasted_iota(jnp.int32, queries.shape, 1)
    own = jnp.where((lane // QK_DIM) == m, queries, jnp.zeros_like(queries))
    return bias + lax.dot_general(
        own, k_all[...], (((1,), (1,)), ((), ())), preferred_element_type=F32
    )


def repeat(count, one):
    if count <= 4:
        for j in range(count):
            one(j, 0)
    else:
        lax.fori_loop(0, count, one, 0)


def attend_first_body(number, pad, tile, inner, *refs):
    q_refs, kv_refs = refs[:inner], refs[inner:-6]
    top_ref, sum_ref, mix_ref, q_all, k_all, v_all = refs[-6:]
    for j in range(inner):
        q_all[j] = q_refs[j][...]
    bias = gather_pieces([(v, tile) for v in kv_refs], k_all, v_all, number, pad)

    def one(j, carry):
        for m in range(2):
            scores = score(q_all, j, m, k_all, bias)
            highest = jnp.max(scores, axis=-1, keepdims=True)
            weights = jnp.exp(scores - highest)
            top_ref[j, m] = highest
            sum_ref[j, m] = jnp.sum(weights, axis=-1, keepdims=True)
            mix_ref[j, m] = jnp.dot(
                weights.astype(BF16), v_all[...], preferred_element_type=F32
            )
        return carry

    repeat(inner, one)


def attend_last_body(number, pad, tile, outer, inner, *refs):
    factor_ref, top_ref, sum_ref, mix_ref = refs[:4]
    q_refs, kv_refs = refs[4 : 4 + inner], refs[4 + inner : -4]
    out_ref, q_all, k_all, v_all = refs[-4:]
    for j in range(inner):
        q_all[j] = q_refs[j][...]
    bias = gather_pieces([(v, tile) for v in kv_refs], k_all, v_all, number, pad)

    def one(j, carry):
        mixed = []
        for m in range(2):
            scores = score(q_all, j, m, k_all, bias)
            before = top_ref[j, m]
            highest = jnp.maximum(before, jnp.max(scores, axis=-1, keepdims=True))
            fade = jnp.exp(before - highest)
            weights = jnp.exp(scores - highest)
            totals = sum_ref[j, m] * fade + jnp.sum(weights, axis=-1, keepdims=True)
            mix = mix_ref[j, m] * fade + jnp.dot(
                weights.astype(BF16), v_all[...], preferred_element_type=F32
            )
            mixed.append(mix / totals)
        head = mixed[0] - factor_ref[0] * mixed[1]
        head = head * lax.rsqrt(jnp.mean(head * head, axis=-1, keepdims=True) + HEAD_EPS)
        head = head.astype(BF16)
        for k in range(outer):
            out_ref[k, j] = head[k * pad : (k + 1) * pad]
        return carry

    repeat(inner, one)


def partial_out_body(singles, pairs, inner, pad, *refs):
    side_ref = refs[0]
    alone = refs[1 : 2 + len(singles)]
    paired = refs[2 + len(singles) : 2 + len(singles) + 2 * len(pairs)]
    rest = refs[2 + len(singles) + 2 * len(pairs) :]
    outer = 1 + len(singles) + 2 * len(pairs)
    parts, own_ref, others = rest[:outer], rest[outer], rest[1 + outer :]
    rows = inner * pad

    def part(k):
        return parts[k][...].reshape(rows, VAL_DIM)

    terms = [(part(0), alone[0])] + [(part(k), w) for k, w in zip(singles, alone[1:])]
    first = jnp.broadcast_to(side_ref[0], (rows, VAL_DIM)) == 0
    for i, (a, b) in enumerate(pairs):
        terms.append((jnp.where(first, part(a), part(b)), paired[2 * i]))
        terms.append((jnp.where(first, part(b), part(a)), paired[2 * i + 1]))
    total = None
    for rows_in, weight in terms:
        term = jnp.dot(rows_in, weight[...], preferred_element_type=F32)
        total = term if total is None else total + term
    own_ref[...] = total[:pad]
    for j in range(1, inner):
        others[j - 1][...] = total[j * pad : (j + 1) * pad].astype(BF16)


def final_body(count, *refs):
    latent_ref, mod_ref, own_ref = refs[:3]
    others = refs[3 : 3 + count]
    out_ref = refs[3 + count]
    number, width = out_ref.shape
    total = own_ref[...]
    for other in others:
        total = total + other[...].astype(F32)
    total = total[:number]
    total = total * lax.rsqrt(jnp.mean(total * total, axis=-1, keepdims=True) + NORM_EPS)
    gate = mod_ref[0:1, 2 * width :]
    out_ref[...] = (latent_ref[...].astype(F32) + gate * total).astype(BF16)


def shards(
    latent,
    context,
    cond_latent,
    cond_context,
    mod_weight,
    w_query,
    w_key,
    w_value,
    w_out,
    head_lambda,
):
    number, width = latent.shape
    groups, ranks = lax.axis_size("sp"), lax.axis_size("tp")
    outer, inner = split_of(ranks)
    pad = -(-number // 16) * 16
    wide = 2 * QK_DIM
    tile = outer * pad
    held = context.shape[0]
    here_sp, here_tp = lax.axis_index("sp"), lax.axis_index("tp")

    def along_outer(value, k, way):
        pairs = [
            (o * inner + i, way(o, k, outer) * inner + i)
            for o in range(outer)
            for i in range(inner)
        ]
        return lax.ppermute(value, "tp", pairs)

    def along_inner(value, j, way):
        pairs = [
            (o * inner + i, o * inner + way(i, j, inner))
            for o in range(outer)
            for i in range(inner)
        ]
        return lax.ppermute(value, "tp", pairs)

    columns = mod_weight.shape[1]
    copies = call(
        partial_body,
        sds((groups * ranks, 2, columns), F32),
        cond_latent.reshape(1, -1),
        cond_context.reshape(1, -1),
        mod_weight,
        scratch=[
            pltpu.VMEM((2, cond_latent.shape[0]), F32),
            pltpu.VMEM(mod_weight.shape, BF16),
            pltpu.SemaphoreType.DMA((3,)),
        ],
        in_specs=[HBM] * 3,
        local=True,
    )
    pieces = lax.all_to_all(copies, ("sp", "tp"), 0, 0)

    blocks = {(0, 0): latent}
    for k in range(1, outer):
        blocks[k, 0] = along_outer(latent, k, ahead)
    for j in range(1, inner):
        for k in range(outer):
            blocks[k, j] = along_inner(blocks[k, 0], j, ahead)

    here = (here_sp * ranks + here_tp).astype(jnp.int32).reshape(1)
    joined = wide + wide + VAL_DIM
    table, weight = call(
        functools.partial(table_body, number, pad, ranks, outer, inner),
        (sds((inner, 2, tile, wide), F32), sds((width, joined), BF16)),
        here,
        w_query,
        w_key,
        w_value,
        scratch=[pltpu.SemaphoreType.DMA((3,))],
        in_specs=[SMEM] + [HBM] * 3,
        local=True,
    )
    mod, q_first, kv_first = call(
        functools.partial(first_body, pad, ranks, outer),
        (
            sds((2, columns * ranks), F32),
            sds((tile, wide), BF16),
            sds((tile + held, wide + VAL_DIM), BF16),
        ),
        pieces,
        context,
        table,
        weight,
        *[blocks[k, 0] for k in range(outer)],
        scratch=[pltpu.VMEM((tile, width), BF16), pltpu.VMEM((held, width), BF16)],
        in_specs=[VMEM] * 5 + [NEAR] * (outer - 1),
    )
    queries, kv = [q_first], [kv_first]
    for j in range(1, inner):
        q_next, kv_next = call(
            functools.partial(second_body, pad, outer, j),
            (sds((tile, wide), BF16), sds((tile, wide + VAL_DIM), BF16)),
            mod,
            table,
            weight,
            *[blocks[k, j] for k in range(outer)],
            scratch=[pltpu.VMEM((tile, width), BF16)],
            in_specs=[VMEM] * 3 + [NEAR] * outer,
        )
        queries.append(q_next)
        kv.append(kv_next)
    share = share_of(groups)
    lines = groups // share

    def along_lines(value, s):
        pairs = [
            (g * share + c, ahead(g, s, lines) * share + c)
            for g in range(lines)
            for c in range(share)
        ]
        return lax.ppermute(value, "sp", pairs)

    swap = [(i, i ^ 1) for i in range(groups)]

    def spread(part):
        pieces = [part]
        for s in range(1, lines):
            pieces.append(along_lines(part, s))
        if share > 1:
            for piece in list(pieces):
                pieces.append(lax.ppermute(piece, "sp", swap))
        return pieces

    kv = [spread(part) for part in kv]
    early, late = kv[0], sum(kv[1:], [])
    stats = (
        sds((inner, 2, tile, 1), F32),
        sds((inner, 2, tile, 1), F32),
        sds((inner, 2, tile, VAL_DIM), F32),
    )

    def room(keys):
        return [
            pltpu.VMEM((inner, tile, wide), BF16),
            pltpu.VMEM((keys, wide), BF16),
            pltpu.VMEM((keys, VAL_DIM), BF16),
        ]

    keys = groups * (tile + held)
    first_stats = call(
        functools.partial(attend_first_body, number, pad, tile, inner),
        stats,
        *queries,
        *early,
        scratch=room(keys),
        extra=tile * keys * 12,
    )
    keys = groups * (inner - 1) * tile
    attended = call(
        functools.partial(attend_last_body, number, pad, tile, outer, inner),
        sds((outer, inner, pad, VAL_DIM), BF16),
        head_lambda,
        *first_stats,
        *queries,
        *late,
        scratch=room(keys),
        extra=tile * keys * 12,
        in_specs=[SMEM] + [VMEM] * (3 + inner + len(late)),
    )
    parts = [attended[0]]
    for k in range(1, outer):
        parts.append(along_outer(attended[k], k, behind))

    singles, pairs = plan(groups, outer)
    side = here_sp % share
    alone, paired = [], []
    for k in singles:
        alone.append(along_outer(w_out, k, behind))
    for a, b in pairs:
        moves = [
            (
                (s * outer + o) * inner + i,
                (s * outer + behind(o, b if s % 2 else a, outer)) * inner + i,
            )
            for s in range(groups)
            for o in range(outer)
            for i in range(inner)
        ]
        paired.append(lax.ppermute(w_out, ("sp", "tp"), moves))
        paired.append(lax.ppermute(paired[-1], "sp", swap))
    total = call(
        functools.partial(partial_out_body, singles, pairs, inner, pad),
        (sds((pad, width), F32),) + (sds((pad, width), BF16),) * (inner - 1),
        side.reshape(1).astype(jnp.int32),
        w_out,
        *alone,
        *paired,
        *parts,
        in_specs=[SMEM, VMEM] + [NEAR] * (len(alone) + len(paired)) + [VMEM] * outer,
    )
    arrived = []
    for j in range(1, inner):
        arrived.append(along_inner(total[j], j, behind))
    return call(
        functools.partial(final_body, inner - 1),
        sds((number, width), BF16),
        latent,
        mod,
        total[0],
        *arrived,
    )


def share_of(groups):
    return 2 if groups % 2 == 0 else 1


def plan(groups, outer):
    if share_of(groups) == 1:
        return tuple(range(1, outer)), ()
    pairs = tuple((k, k + 1) for k in range(2, outer - 1, 2))
    paired = {k for pair in pairs for k in pair}
    return tuple(k for k in range(1, outer) if k not in paired), pairs


def solution(mesh):
    placed = (
        P(("sp", "tp"), None),
        P("sp", None),
        P("sp"),
        P("sp"),
        P("sp", "tp"),
        P(None, "tp"),
        P(None, "tp"),
        P(None, "tp"),
        P("tp", None),
        P("tp"),
    )
    return jax.shard_map(
        shards, mesh=mesh, in_specs=placed, out_specs=P(("sp", "tp"), None), check_vma=False
    )
```

```python
import functools

import jax
import jax.numpy as jnp
import numpy as np
from jax import lax
from jax.experimental import pallas as pl
from jax.experimental.pallas import tpu as pltpu
from jax.sharding import PartitionSpec as P

QK_DIM = 64
VAL_DIM = 128
GRID_W = 64

NORM_EPS = 0.01
HEAD_EPS = 0.001
THETA = 10000.0

F32 = jnp.float32
BF16 = jnp.bfloat16
VMEM = pl.BlockSpec(memory_space=pltpu.VMEM)
SMEM = pl.BlockSpec(memory_space=pltpu.SMEM)
NEAR = pl.BlockSpec(memory_space=pltpu.VMEM)
HBM = pl.BlockSpec(memory_space=pltpu.HBM)


def ahead(i, k, n):
    return i ^ k if n & (n - 1) == 0 else (i + k) % n


def behind(i, k, n):
    return i ^ k if n & (n - 1) == 0 else (i - k) % n


def split_of(size):
    inner = max(d for d in range(1, size + 1) if size % d == 0 and d * d <= size)
    return size // inner, inner


def size_of(v):
    return int(np.prod(v.shape)) * jnp.dtype(v.dtype).itemsize


def call(body, outs, *args, scratch=(), extra=0, local=False, flops=2000000, in_specs=None):
    held = sum(size_of(v) for v in args) + sum(size_of(v) for v in jax.tree.leaves(outs))
    held += sum(size_of(v) for v in scratch if hasattr(v, "dtype") and v.dtype in (F32, BF16))
    limit = min(60 * 1024 * 1024, held + extra + 6 * 1024 * 1024)
    in_specs = in_specs or [VMEM] * len(args)
    args = [
        pltpu.with_memory_space_constraint(v, pltpu.HBM)
        if spec is HBM
        else pltpu.with_memory_space_constraint(v, pltpu.VMEM)
        if spec is NEAR
        else v
        for v, spec in zip(args, in_specs)
    ]
    if local:
        outs = jax.tree.map(lambda v: pltpu.VMEM(v.shape, v.dtype), outs)
    return pl.pallas_call(
        body,
        out_shape=outs,
        in_specs=in_specs,
        out_specs=jax.tree.map(lambda _: VMEM, outs),
        scratch_shapes=list(scratch),
        compiler_params=pltpu.CompilerParams(vmem_limit_bytes=limit),
        cost_estimate=pl.CostEstimate(flops=flops, bytes_accessed=0, transcendentals=0),
    )(*args)


def sds(shape, dtype):
    return jax.ShapeDtypeStruct(shape, dtype)


def partial_body(latent_hbm, context_hbm, weight_hbm, out_ref, cond_ref, weight_ref, sems):
    moves = [
        pltpu.make_async_copy(weight_hbm, weight_ref, sems.at[0]),
        pltpu.make_async_copy(latent_hbm, cond_ref.at[0:1], sems.at[1]),
        pltpu.make_async_copy(context_hbm, cond_ref.at[1:2], sems.at[2]),
    ]
    for move in moves:
        move.start()
    moves[1].wait()
    moves[2].wait()
    rows = cond_ref[...]
    rows = (rows / (1.0 + jnp.exp(-rows))).astype(BF16)
    moves[0].wait()
    part = jnp.dot(rows, weight_ref[...], preferred_element_type=F32)
    for i in range(out_ref.shape[0]):
        out_ref[i] = part


def table_body(number, pad, ranks, outer, inner, *refs):
    here_ref = refs[0]
    sources, (out_ref, weight_ref, sems) = refs[1:4], refs[4:]
    moves = fetch_weights(sources, weight_ref, sems)
    here = here_ref[0]
    group, rank = lax.div(here, ranks), lax.rem(here, ranks)
    here_outer, here_inner = lax.div(rank, inner), lax.rem(rank, inner)
    lane = lax.broadcasted_iota(jnp.int32, (pad, 2 * QK_DIM), 1)
    line = lax.broadcasted_iota(jnp.int32, (pad, 2 * QK_DIM), 0)
    low = lane < QK_DIM
    by_row = (lane & (QK_DIM - 1)) < QK_DIM // 2
    sign = jnp.where((lane & (QK_DIM // 4)) == 0, -1.0, 1.0)
    phase = jnp.where(low, np.float32(np.pi / 2), np.float32(0))
    shift = GRID_W.bit_length() - 1
    quarter = QK_DIM // 4
    inverse = jnp.ones(lane.shape, F32)
    for i in range(1, quarter):
        inverse = jnp.where((lane & (quarter - 1)) == i, np.float32(THETA ** (-i / quarter)), inverse)

    def owner(i, k, n):
        return i ^ k if n & (n - 1) == 0 else lax.rem(i + (n - k), n)

    for j in range(inner):
        for k in range(outer):
            rank_at = owner(here_outer, k, outer) * inner + owner(here_inner, j, inner)
            position = line + (group * ranks + rank_at) * number
            place = jnp.where(by_row, position >> shift, position & (GRID_W - 1)).astype(F32)
            wave = jnp.sin(place * inverse + phase)
            other = pltpu.roll(wave, QK_DIM, 1)
            out_ref[j, 0, k * pad : (k + 1) * pad, :] = jnp.where(low, wave, other)
            out_ref[j, 1, k * pad : (k + 1) * pad, :] = jnp.where(low, other, wave) * sign
    for move in moves:
        move.wait()


def fetch_weights(sources, weight_ref, sems):
    moves, start = [], 0
    for i, source in enumerate(sources):
        columns = source.shape[1]
        moves.append(
            pltpu.make_async_copy(source, weight_ref.at[:, start : start + columns], sems.at[i])
        )
        moves[-1].start()
        start += columns
    return moves


def modulated(values, shift, scale):
    values = values.astype(F32)
    mean = jnp.mean(values * values, axis=-1, keepdims=True)
    return (values * lax.rsqrt(mean + NORM_EPS) * scale + shift).astype(BF16)


def fill_rows(blocks, rows_ref, pad, shift, scale):
    number = blocks[0].shape[0]
    for k, block in enumerate(blocks):
        rows_ref[k * pad : k * pad + number, :] = modulated(block[...], shift, scale)
        if pad > number:
            rows_ref[k * pad + number : (k + 1) * pad, :] = jnp.zeros(
                (pad - number, rows_ref.shape[1]), BF16
            )


def turn(u, cosine, sine):
    lane = lax.broadcasted_iota(jnp.int32, u.shape, 1)
    quarter = QK_DIM // 4
    width = u.shape[1]
    even = (lane // quarter) % 2 == 0
    turned = jnp.where(even, pltpu.roll(u, width - quarter, 1), pltpu.roll(u, quarter, 1))
    return (u * cosine + turned * sine).astype(BF16)


def project_rows(rows, weight_ref, table_ref, j, q_ref, kv_ref):
    number = rows.shape[0]
    wide = 2 * QK_DIM
    cosine, sine = table_ref[j, 0], table_ref[j, 1]
    u = jnp.dot(rows, weight_ref[...], preferred_element_type=F32)
    q_ref[...] = turn(u[:, :wide], cosine, sine)
    kv_ref[0:number, :wide] = turn(u[:, wide : 2 * wide], cosine, sine)
    kv_ref[0:number, wide:] = u[:, 2 * wide :].astype(BF16)


def first_body(pad, ranks, count, *refs):
    pieces_ref, context_hbm, table_ref, weight_ref = refs[:4]
    blocks = refs[4 : 4 + count]
    mod_ref, q_ref, kv_ref, rows_ref, context_ref, sem = refs[4 + count :]
    move = pltpu.make_async_copy(context_hbm, context_ref, sem)
    move.start()
    width = context_ref.shape[1]
    columns = pieces_ref.shape[2]
    groups = pieces_ref.shape[0] // ranks
    for t in range(ranks):
        total = pieces_ref[t]
        for s in range(1, groups):
            total = total + pieces_ref[s * ranks + t]
        mod_ref[:, t * columns : (t + 1) * columns] = total
    mod = mod_ref[...]
    fill_rows(blocks, rows_ref, pad, mod[0:1, :width], 1.0 + mod[0:1, width : 2 * width])
    project_rows(rows_ref[...], weight_ref, table_ref, 0, q_ref, kv_ref)
    shift, scale = mod[1:2, :width], 1.0 + mod[1:2, width : 2 * width]
    held = context_ref.shape[0]
    step = 16 if held % 16 == 0 else held
    move.wait()
    for i in range(0, held, step):
        context_ref[i : i + step, :] = modulated(context_ref[i : i + step, :], shift, scale)
    base = count * pad
    wide = 2 * QK_DIM
    kv_ref[base : base + held, :] = jnp.dot(
        context_ref[...], weight_ref[:, wide:], preferred_element_type=F32
    ).astype(BF16)


def second_body(pad, count, j, *refs):
    mod_ref, table_ref, weight_ref = refs[:3]
    blocks = refs[3 : 3 + count]
    q_ref, kv_ref, rows_ref = refs[3 + count :]
    width = blocks[0].shape[1]
    fill_rows(
        blocks, rows_ref, pad, mod_ref[0:1, :width], 1.0 + mod_ref[0:1, width : 2 * width]
    )
    project_rows(rows_ref[...], weight_ref, table_ref, j, q_ref, kv_ref)


def gather_pieces(pieces, k_all, v_all, number, pad):
    wide = 2 * QK_DIM
    row = 0
    for piece, rows in pieces:
        k_all[row : row + rows, :] = piece[0:rows, :wide]
        v_all[row : row + rows, :] = piece[0:rows, wide:]
        row += rows
    latents = row
    for piece, rows in pieces:
        held = piece.shape[0] - rows
        if held:
            k_all[row : row + held, :] = piece[rows : rows + held, :wide]
            v_all[row : row + held, :] = piece[rows : rows + held, wide:]
            row += held
    column = lax.broadcasted_iota(jnp.int32, (1, row), 1)
    valid = (column >= latents) | (column % pad < number)
    return jnp.where(valid, 0.0, -1e30)


def score(q_all, j, m, k_all, bias):
    queries = q_all[j] * jnp.asarray(QK_DIM ** (-0.5), BF16)
    lane = lax.broadcasted_iota(jnp.int32, queries.shape, 1)
    own = jnp.where((lane // QK_DIM) == m, queries, jnp.zeros_like(queries))
    return bias + lax.dot_general(
        own, k_all[...], (((1,), (1,)), ((), ())), preferred_element_type=F32
    )


def repeat(count, one):
    if count <= 4:
        for j in range(count):
            one(j, 0)
    else:
        lax.fori_loop(0, count, one, 0)


def attend_first_body(number, pad, tile, inner, *refs):
    q_refs, kv_refs = refs[:inner], refs[inner:-6]
    top_ref, sum_ref, mix_ref, q_all, k_all, v_all = refs[-6:]
    for j in range(inner):
        q_all[j] = q_refs[j][...]
    bias = gather_pieces([(v, tile) for v in kv_refs], k_all, v_all, number, pad)

    def one(j, carry):
        for m in range(2):
            scores = score(q_all, j, m, k_all, bias)
            highest = jnp.max(scores, axis=-1, keepdims=True)
            weights = jnp.exp(scores - highest)
            top_ref[j, m] = highest
            sum_ref[j, m] = jnp.sum(weights, axis=-1, keepdims=True)
            mix_ref[j, m] = jnp.dot(
                weights.astype(BF16), v_all[...], preferred_element_type=F32
            )
        return carry

    repeat(inner, one)


def attend_last_body(number, pad, tile, outer, inner, *refs):
    factor_ref, top_ref, sum_ref, mix_ref = refs[:4]
    q_refs, kv_refs = refs[4 : 4 + inner], refs[4 + inner : -4]
    out_ref, q_all, k_all, v_all = refs[-4:]
    for j in range(inner):
        q_all[j] = q_refs[j][...]
    bias = gather_pieces([(v, tile) for v in kv_refs], k_all, v_all, number, pad)

    def one(j, carry):
        mixed = []
        for m in range(2):
            scores = score(q_all, j, m, k_all, bias)
            before = top_ref[j, m]
            highest = jnp.maximum(before, jnp.max(scores, axis=-1, keepdims=True))
            fade = jnp.exp(before - highest)
            weights = jnp.exp(scores - highest)
            totals = sum_ref[j, m] * fade + jnp.sum(weights, axis=-1, keepdims=True)
            mix = mix_ref[j, m] * fade + jnp.dot(
                weights.astype(BF16), v_all[...], preferred_element_type=F32
            )
            mixed.append(mix / totals)
        head = mixed[0] - factor_ref[0] * mixed[1]
        head = head * lax.rsqrt(jnp.mean(head * head, axis=-1, keepdims=True) + HEAD_EPS)
        head = head.astype(BF16)
        for k in range(outer):
            out_ref[k, j] = head[k * pad : (k + 1) * pad]
        return carry

    repeat(inner, one)


def partial_out_body(slots, share, ranks, inner, pad, *refs):
    here_ref, own_hbm = refs[:2]
    held = refs[2 : 2 + len(slots)]
    rest = refs[2 + len(slots) : -2]
    own_weight, sem = refs[-2:]
    move = pltpu.make_async_copy(own_hbm, own_weight, sem)
    move.start()
    outer = 1 + len(slots)
    parts, own_ref, others = rest[:outer], rest[outer], rest[1 + outer :]
    rows = inner * pad
    side = lax.rem(lax.div(here_ref[0], ranks), share)
    first = jnp.broadcast_to(side, (rows, VAL_DIM)) == 0

    def part(k):
        return parts[k][...].reshape(rows, VAL_DIM)

    total = None
    for (a, b), weight in zip(slots, held):
        rows_in = part(a) if a == b else jnp.where(first, part(a), part(b))
        term = jnp.dot(rows_in, weight[...], preferred_element_type=F32)
        total = term if total is None else total + term
    move.wait()
    total += jnp.dot(part(0), own_weight[...], preferred_element_type=F32)
    own_ref[...] = total[:pad]
    for j in range(1, inner):
        others[j - 1][...] = total[j * pad : (j + 1) * pad].astype(BF16)


def final_body(count, *refs):
    latent_ref, mod_ref, own_ref = refs[:3]
    others = refs[3 : 3 + count]
    out_ref = refs[3 + count]
    number, width = out_ref.shape
    total = own_ref[...]
    for other in others:
        total = total + other[...].astype(F32)
    total = total[:number]
    total = total * lax.rsqrt(jnp.mean(total * total, axis=-1, keepdims=True) + NORM_EPS)
    gate = mod_ref[0:1, 2 * width :]
    out_ref[...] = (latent_ref[...].astype(F32) + gate * total).astype(BF16)


def shards(
    latent,
    context,
    cond_latent,
    cond_context,
    mod_weight,
    w_query,
    w_key,
    w_value,
    w_out,
    head_lambda,
):
    number, width = latent.shape
    groups, ranks = lax.axis_size("sp"), lax.axis_size("tp")
    outer, inner = split_of(ranks)
    pad = -(-number // 16) * 16
    wide = 2 * QK_DIM
    tile = outer * pad
    held = context.shape[0]
    here_sp, here_tp = lax.axis_index("sp"), lax.axis_index("tp")

    def along_outer(value, k, way):
        pairs = [
            (o * inner + i, way(o, k, outer) * inner + i)
            for o in range(outer)
            for i in range(inner)
        ]
        return lax.ppermute(value, "tp", pairs)

    def along_inner(value, j, way):
        pairs = [
            (o * inner + i, o * inner + way(i, j, inner))
            for o in range(outer)
            for i in range(inner)
        ]
        return lax.ppermute(value, "tp", pairs)

    columns = mod_weight.shape[1]
    copies = call(
        partial_body,
        sds((groups * ranks, 2, columns), F32),
        cond_latent.reshape(1, -1),
        cond_context.reshape(1, -1),
        mod_weight,
        scratch=[
            pltpu.VMEM((2, cond_latent.shape[0]), F32),
            pltpu.VMEM(mod_weight.shape, BF16),
            pltpu.SemaphoreType.DMA((3,)),
        ],
        in_specs=[HBM] * 3,
        local=True,
    )
    pieces = lax.all_to_all(copies, ("sp", "tp"), 0, 0)

    blocks = {(0, 0): latent}
    for k in range(1, outer):
        if relayed(k):
            blocks[k, 0] = along_outer(blocks[k - 1, 0], 1, ahead)
        else:
            blocks[k, 0] = along_outer(latent, k, ahead)
    for j in range(1, inner):
        for k in range(outer):
            blocks[k, j] = along_inner(blocks[k, 0], j, ahead)

    here = (here_sp * ranks + here_tp).astype(jnp.int32).reshape(1)
    joined = wide + wide + VAL_DIM
    table, weight = call(
        functools.partial(table_body, number, pad, ranks, outer, inner),
        (sds((inner, 2, tile, wide), F32), sds((width, joined), BF16)),
        here,
        w_query,
        w_key,
        w_value,
        scratch=[pltpu.SemaphoreType.DMA((3,))],
        in_specs=[SMEM] + [HBM] * 3,
        local=True,
    )
    mod, q_first, kv_first = call(
        functools.partial(first_body, pad, ranks, outer),
        (
            sds((2, columns * ranks), F32),
            sds((tile, wide), BF16),
            sds((tile + held, wide + VAL_DIM), BF16),
        ),
        pieces,
        context,
        table,
        weight,
        *[blocks[k, 0] for k in range(outer)],
        scratch=[
            pltpu.VMEM((tile, width), BF16),
            pltpu.VMEM((held, width), BF16),
            pltpu.SemaphoreType.DMA,
        ],
        in_specs=[VMEM, HBM] + [VMEM] * (2 + outer),
    )
    queries, kv = [q_first], [kv_first]
    for j in range(1, inner):
        q_next, kv_next = call(
            functools.partial(second_body, pad, outer, j),
            (sds((tile, wide), BF16), sds((tile, wide + VAL_DIM), BF16)),
            mod,
            table,
            weight,
            *[blocks[k, j] for k in range(outer)],
            scratch=[pltpu.VMEM((tile, width), BF16)],
        )
        queries.append(q_next)
        kv.append(kv_next)
    share = share_of(groups)
    lines = groups // share

    def along_lines(value, s):
        pairs = [
            (g * share + c, ahead(g, s, lines) * share + c)
            for g in range(lines)
            for c in range(share)
        ]
        return lax.ppermute(value, "sp", pairs)

    swap = [(i, i ^ 1) for i in range(groups)]

    def spread(part):
        pieces = [part]
        for s in range(1, lines):
            pieces.append(along_lines(part, s))
        if share > 1:
            for piece in list(pieces):
                pieces.append(lax.ppermute(piece, "sp", swap))
        return pieces

    kv = [spread(part) for part in kv]
    early, late = kv[0], sum(kv[1:], [])
    stats = (
        sds((inner, 2, tile, 1), F32),
        sds((inner, 2, tile, 1), F32),
        sds((inner, 2, tile, VAL_DIM), F32),
    )

    def room(keys):
        return [
            pltpu.VMEM((inner, tile, wide), BF16),
            pltpu.VMEM((keys, wide), BF16),
            pltpu.VMEM((keys, VAL_DIM), BF16),
        ]

    keys = groups * (tile + held)
    first_stats = call(
        functools.partial(attend_first_body, number, pad, tile, inner),
        stats,
        *queries,
        *early,
        scratch=room(keys),
        extra=tile * keys * 12,
    )
    keys = groups * (inner - 1) * tile
    attended = call(
        functools.partial(attend_last_body, number, pad, tile, outer, inner),
        sds((outer, inner, pad, VAL_DIM), BF16),
        head_lambda,
        *first_stats,
        *queries,
        *late,
        scratch=room(keys),
        extra=tile * keys * 12,
        in_specs=[SMEM] + [VMEM] * (3 + inner + len(late)),
    )
    parts = [attended[0]]
    for k in range(1, outer):
        parts.append(along_outer(attended[k], k, behind))

    def joint(value, target):
        moves = []
        for s in range(groups):
            for o in range(outer):
                for i in range(inner):
                    to_s, to_o = target(s, o)
                    moves.append(
                        ((s * outer + o) * inner + i, (to_s * outer + to_o) * inner + i)
                    )
        return lax.ppermute(value, ("sp", "tp"), moves)

    slots, weights = [], []
    if share > 1 and outer == 4:
        fetched = joint(w_out, lambda s, o: (s, behind(o, 1 if s % 2 else 2, outer)))
        turned = joint(fetched, lambda s, o: (s ^ 1, o if s % 2 else behind(o, 1, outer)))
        given = jnp.where(here_sp % 2 == 0, fetched, turned)
        traded = lax.ppermute(given, "sp", swap)
        slots, weights = [(2, 1), (1, 3), (3, 2)], [fetched, turned, traded]
    else:
        for k in range(1, outer):
            weights.append(along_outer(w_out, k, behind))
            slots.append((k, k))
    depth = w_out.shape[0]
    total = call(
        functools.partial(partial_out_body, slots, share, ranks, inner, pad),
        (sds((pad, width), F32),) + (sds((pad, width), BF16),) * (inner - 1),
        here,
        w_out,
        *weights,
        *parts,
        scratch=[pltpu.VMEM((depth, width), BF16), pltpu.SemaphoreType.DMA],
        in_specs=[SMEM, HBM] + [VMEM] * (len(weights) + outer),
    )
    arrived = []
    for j in range(1, inner):
        arrived.append(along_inner(total[j], j, behind))
    return call(
        functools.partial(final_body, inner - 1),
        sds((number, width), BF16),
        latent,
        mod,
        total[0],
        *arrived,
    )


def relayed(k):
    return k > 1 and k % 2 == 1


def share_of(groups):
    return 2 if groups % 2 == 0 else 1


def solution(mesh):
    placed = (
        P(("sp", "tp"), None),
        P("sp", None),
        P("sp"),
        P("sp"),
        P("sp", "tp"),
        P(None, "tp"),
        P(None, "tp"),
        P(None, "tp"),
        P("tp", None),
        P("tp"),
    )
    return jax.shard_map(
        shards, mesh=mesh, in_specs=placed, out_specs=P(("sp", "tp"), None), check_vma=False
    )
```

```python
import functools

import jax
import jax.numpy as jnp
import numpy as np
from jax import lax
from jax.experimental import pallas as pl
from jax.experimental.pallas import tpu as pltpu
from jax.sharding import PartitionSpec as P

QK_DIM = 64
VAL_DIM = 128
GRID_W = 64

NORM_EPS = 0.01
HEAD_EPS = 0.001
THETA = 10000.0

F32 = jnp.float32
BF16 = jnp.bfloat16
VMEM = pl.BlockSpec(memory_space=pltpu.VMEM)
SMEM = pl.BlockSpec(memory_space=pltpu.SMEM)
NEAR = pl.BlockSpec(memory_space=pltpu.VMEM)
HBM = pl.BlockSpec(memory_space=pltpu.HBM)


def ahead(i, k, n):
    return i ^ k if n & (n - 1) == 0 else (i + k) % n


def behind(i, k, n):
    return i ^ k if n & (n - 1) == 0 else (i - k) % n


def split_of(size):
    inner = max(d for d in range(1, size + 1) if size % d == 0 and d * d <= size)
    return size // inner, inner


def size_of(v):
    return int(np.prod(v.shape)) * jnp.dtype(v.dtype).itemsize


def call(body, outs, *args, scratch=(), extra=0, local=False, flops=2000000, in_specs=None):
    held = sum(size_of(v) for v in args) + sum(size_of(v) for v in jax.tree.leaves(outs))
    held += sum(size_of(v) for v in scratch if hasattr(v, "dtype") and v.dtype in (F32, BF16))
    limit = min(60 * 1024 * 1024, held + extra + 6 * 1024 * 1024)
    in_specs = in_specs or [VMEM] * len(args)
    args = [
        pltpu.with_memory_space_constraint(v, pltpu.HBM)
        if spec is HBM
        else pltpu.with_memory_space_constraint(v, pltpu.VMEM)
        if spec is NEAR
        else v
        for v, spec in zip(args, in_specs)
    ]
    if local:
        outs = jax.tree.map(lambda v: pltpu.VMEM(v.shape, v.dtype), outs)
    return pl.pallas_call(
        body,
        out_shape=outs,
        in_specs=in_specs,
        out_specs=jax.tree.map(lambda _: VMEM, outs),
        scratch_shapes=list(scratch),
        compiler_params=pltpu.CompilerParams(vmem_limit_bytes=limit),
        cost_estimate=pl.CostEstimate(flops=flops, bytes_accessed=0, transcendentals=0),
    )(*args)


def sds(shape, dtype):
    return jax.ShapeDtypeStruct(shape, dtype)


def partial_body(latent_hbm, context_hbm, weight_hbm, out_ref, cond_ref, weight_ref, sems):
    moves = [
        pltpu.make_async_copy(weight_hbm, weight_ref, sems.at[0]),
        pltpu.make_async_copy(latent_hbm, cond_ref.at[0:1], sems.at[1]),
        pltpu.make_async_copy(context_hbm, cond_ref.at[1:2], sems.at[2]),
    ]
    for move in moves:
        move.start()
    moves[1].wait()
    moves[2].wait()
    rows = cond_ref[...]
    rows = (rows / (1.0 + jnp.exp(-rows))).astype(BF16)
    moves[0].wait()
    part = jnp.dot(rows, weight_ref[...], preferred_element_type=F32)
    part = part.astype(BF16)
    for i in range(out_ref.shape[0]):
        out_ref[i] = part


def table_body(number, pad, ranks, outer, inner, *refs):
    here_ref = refs[0]
    sources, (out_ref, weight_ref, sems) = refs[1:4], refs[4:]
    moves = fetch_weights(sources, weight_ref, sems)
    here = here_ref[0]
    group, rank = lax.div(here, ranks), lax.rem(here, ranks)
    here_outer, here_inner = lax.div(rank, inner), lax.rem(rank, inner)
    lane = lax.broadcasted_iota(jnp.int32, (pad, 2 * QK_DIM), 1)
    line = lax.broadcasted_iota(jnp.int32, (pad, 2 * QK_DIM), 0)
    low = lane < QK_DIM
    by_row = (lane & (QK_DIM - 1)) < QK_DIM // 2
    sign = jnp.where((lane & (QK_DIM // 4)) == 0, -1.0, 1.0)
    phase = jnp.where(low, np.float32(np.pi / 2), np.float32(0))
    shift = GRID_W.bit_length() - 1
    quarter = QK_DIM // 4
    inverse = jnp.ones(lane.shape, F32)
    for i in range(1, quarter):
        inverse = jnp.where((lane & (quarter - 1)) == i, np.float32(THETA ** (-i / quarter)), inverse)

    def owner(i, k, n):
        return i ^ k if n & (n - 1) == 0 else lax.rem(i + (n - k), n)

    for j in range(inner):
        for k in range(outer):
            rank_at = owner(here_outer, k, outer) * inner + owner(here_inner, j, inner)
            position = line + (group * ranks + rank_at) * number
            place = jnp.where(by_row, position >> shift, position & (GRID_W - 1)).astype(F32)
            wave = jnp.sin(place * inverse + phase)
            other = pltpu.roll(wave, QK_DIM, 1)
            out_ref[j, 0, k * pad : (k + 1) * pad, :] = jnp.where(low, wave, other)
            out_ref[j, 1, k * pad : (k + 1) * pad, :] = jnp.where(low, other, wave) * sign
    for move in moves:
        move.wait()


def fetch_weights(sources, weight_ref, sems):
    moves, start = [], 0
    for i, source in enumerate(sources):
        columns = source.shape[1]
        moves.append(
            pltpu.make_async_copy(source, weight_ref.at[:, start : start + columns], sems.at[i])
        )
        moves[-1].start()
        start += columns
    return moves


def modulated(values, shift, scale):
    values = values.astype(F32)
    mean = jnp.mean(values * values, axis=-1, keepdims=True)
    return (values * lax.rsqrt(mean + NORM_EPS) * scale + shift).astype(BF16)


def fill_rows(blocks, rows_ref, pad, shift, scale):
    number = blocks[0].shape[0]
    for k, block in enumerate(blocks):
        rows_ref[k * pad : k * pad + number, :] = modulated(block[...], shift, scale)
        if pad > number:
            rows_ref[k * pad + number : (k + 1) * pad, :] = jnp.zeros(
                (pad - number, rows_ref.shape[1]), BF16
            )


def turn(u, cosine, sine):
    lane = lax.broadcasted_iota(jnp.int32, u.shape, 1)
    quarter = QK_DIM // 4
    width = u.shape[1]
    even = (lane // quarter) % 2 == 0
    turned = jnp.where(even, pltpu.roll(u, width - quarter, 1), pltpu.roll(u, quarter, 1))
    return (u * cosine + turned * sine).astype(BF16)


def project_rows(rows, weight_ref, table_ref, j, q_ref, kv_ref):
    number = rows.shape[0]
    wide = 2 * QK_DIM
    cosine, sine = table_ref[j, 0], table_ref[j, 1]
    u = jnp.dot(rows, weight_ref[...], preferred_element_type=F32)
    q_ref[...] = turn(u[:, :wide], cosine, sine)
    kv_ref[0:number, :wide] = turn(u[:, wide : 2 * wide], cosine, sine)
    kv_ref[0:number, wide:] = u[:, 2 * wide :].astype(BF16)


def first_body(pad, ranks, count, *refs):
    pieces_ref, context_hbm, table_ref, weight_ref = refs[:4]
    blocks = refs[4 : 4 + count]
    mod_ref, q_ref, kv_ref, rows_ref, context_ref, sem = refs[4 + count :]
    move = pltpu.make_async_copy(context_hbm, context_ref, sem)
    move.start()
    width = context_ref.shape[1]
    columns = pieces_ref.shape[2]
    groups = pieces_ref.shape[0] // ranks
    for t in range(ranks):
        total = pieces_ref[t].astype(F32)
        for s in range(1, groups):
            total = total + pieces_ref[s * ranks + t].astype(F32)
        mod_ref[:, t * columns : (t + 1) * columns] = total
    mod = mod_ref[...]
    fill_rows(blocks, rows_ref, pad, mod[0:1, :width], 1.0 + mod[0:1, width : 2 * width])
    project_rows(rows_ref[...], weight_ref, table_ref, 0, q_ref, kv_ref)
    shift, scale = mod[1:2, :width], 1.0 + mod[1:2, width : 2 * width]
    held = context_ref.shape[0]
    step = 16 if held % 16 == 0 else held
    move.wait()
    for i in range(0, held, step):
        context_ref[i : i + step, :] = modulated(context_ref[i : i + step, :], shift, scale)
    base = count * pad
    wide = 2 * QK_DIM
    kv_ref[base : base + held, :] = jnp.dot(
        context_ref[...], weight_ref[:, wide:], preferred_element_type=F32
    ).astype(BF16)


def second_body(pad, count, j, *refs):
    mod_ref, table_ref, weight_ref = refs[:3]
    blocks = refs[3 : 3 + count]
    q_ref, kv_ref, rows_ref = refs[3 + count :]
    width = blocks[0].shape[1]
    fill_rows(
        blocks, rows_ref, pad, mod_ref[0:1, :width], 1.0 + mod_ref[0:1, width : 2 * width]
    )
    project_rows(rows_ref[...], weight_ref, table_ref, j, q_ref, kv_ref)


def gather_pieces(pieces, k_all, v_all, number, pad):
    wide = 2 * QK_DIM
    row = 0
    for piece, rows in pieces:
        k_all[row : row + rows, :] = piece[0:rows, :wide]
        v_all[row : row + rows, :] = piece[0:rows, wide:]
        row += rows
    latents = row
    for piece, rows in pieces:
        held = piece.shape[0] - rows
        if held:
            k_all[row : row + held, :] = piece[rows : rows + held, :wide]
            v_all[row : row + held, :] = piece[rows : rows + held, wide:]
            row += held
    column = lax.broadcasted_iota(jnp.int32, (1, row), 1)
    valid = (column >= latents) | (column % pad < number)
    return jnp.where(valid, 0.0, -1e30)


def score(q_all, j, m, k_all, bias):
    queries = q_all[j] * jnp.asarray(QK_DIM ** (-0.5), BF16)
    lane = lax.broadcasted_iota(jnp.int32, queries.shape, 1)
    own = jnp.where((lane // QK_DIM) == m, queries, jnp.zeros_like(queries))
    return bias + lax.dot_general(
        own, k_all[...], (((1,), (1,)), ((), ())), preferred_element_type=F32
    )


def repeat(count, one):
    if count <= 4:
        for j in range(count):
            one(j, 0)
    else:
        lax.fori_loop(0, count, one, 0)


def attend_first_body(number, pad, tile, inner, *refs):
    q_refs, kv_refs = refs[:inner], refs[inner:-6]
    top_ref, sum_ref, mix_ref, q_all, k_all, v_all = refs[-6:]
    for j in range(inner):
        q_all[j] = q_refs[j][...]
    bias = gather_pieces([(v, tile) for v in kv_refs], k_all, v_all, number, pad)

    def one(j, carry):
        for m in range(2):
            scores = score(q_all, j, m, k_all, bias)
            highest = jnp.max(scores, axis=-1, keepdims=True)
            weights = jnp.exp(scores - highest)
            top_ref[j, m] = highest
            sum_ref[j, m] = jnp.sum(weights, axis=-1, keepdims=True)
            mix_ref[j, m] = jnp.dot(
                weights.astype(BF16), v_all[...], preferred_element_type=F32
            )
        return carry

    repeat(inner, one)


def attend_last_body(number, pad, tile, outer, inner, *refs):
    factor_ref, top_ref, sum_ref, mix_ref = refs[:4]
    q_refs, kv_refs = refs[4 : 4 + inner], refs[4 + inner : -4]
    out_ref, q_all, k_all, v_all = refs[-4:]
    for j in range(inner):
        q_all[j] = q_refs[j][...]
    bias = gather_pieces([(v, tile) for v in kv_refs], k_all, v_all, number, pad)

    def one(j, carry):
        mixed = []
        for m in range(2):
            scores = score(q_all, j, m, k_all, bias)
            before = top_ref[j, m]
            highest = jnp.maximum(before, jnp.max(scores, axis=-1, keepdims=True))
            fade = jnp.exp(before - highest)
            weights = jnp.exp(scores - highest)
            totals = sum_ref[j, m] * fade + jnp.sum(weights, axis=-1, keepdims=True)
            mix = mix_ref[j, m] * fade + jnp.dot(
                weights.astype(BF16), v_all[...], preferred_element_type=F32
            )
            mixed.append(mix / totals)
        head = mixed[0] - factor_ref[0] * mixed[1]
        head = head * lax.rsqrt(jnp.mean(head * head, axis=-1, keepdims=True) + HEAD_EPS)
        head = head.astype(BF16)
        for k in range(outer):
            out_ref[k, j] = head[k * pad : (k + 1) * pad]
        return carry

    repeat(inner, one)


def partial_out_body(slots, share, ranks, inner, pad, *refs):
    here_ref, own_hbm = refs[:2]
    held = refs[2 : 2 + len(slots)]
    rest = refs[2 + len(slots) : -2]
    own_weight, sem = refs[-2:]
    move = pltpu.make_async_copy(own_hbm, own_weight, sem)
    move.start()
    outer = 1 + len(slots)
    parts, own_ref, others = rest[:outer], rest[outer], rest[1 + outer :]
    rows = inner * pad
    side = lax.rem(lax.div(here_ref[0], ranks), share)
    first = jnp.broadcast_to(side, (rows, VAL_DIM)) == 0

    def part(k):
        return parts[k][...].reshape(rows, VAL_DIM)

    total = None
    for (a, b), weight in zip(slots, held):
        rows_in = part(a) if a == b else jnp.where(first, part(a), part(b))
        term = jnp.dot(rows_in, weight[...], preferred_element_type=F32)
        total = term if total is None else total + term
    move.wait()
    total += jnp.dot(part(0), own_weight[...], preferred_element_type=F32)
    own_ref[...] = total[:pad]
    for j in range(1, inner):
        others[j - 1][...] = total[j * pad : (j + 1) * pad].astype(BF16)


def final_body(count, *refs):
    latent_ref, mod_ref, own_ref = refs[:3]
    others = refs[3 : 3 + count]
    out_ref = refs[3 + count]
    number, width = out_ref.shape
    total = own_ref[...]
    for other in others:
        total = total + other[...].astype(F32)
    total = total[:number]
    total = total * lax.rsqrt(jnp.mean(total * total, axis=-1, keepdims=True) + NORM_EPS)
    gate = mod_ref[0:1, 2 * width :]
    out_ref[...] = (latent_ref[...].astype(F32) + gate * total).astype(BF16)


def shards(
    latent,
    context,
    cond_latent,
    cond_context,
    mod_weight,
    w_query,
    w_key,
    w_value,
    w_out,
    head_lambda,
):
    number, width = latent.shape
    groups, ranks = lax.axis_size("sp"), lax.axis_size("tp")
    outer, inner = split_of(ranks)
    pad = -(-number // 16) * 16
    wide = 2 * QK_DIM
    tile = outer * pad
    held = context.shape[0]
    here_sp, here_tp = lax.axis_index("sp"), lax.axis_index("tp")

    def along_outer(value, k, way):
        pairs = [
            (o * inner + i, way(o, k, outer) * inner + i)
            for o in range(outer)
            for i in range(inner)
        ]
        return lax.ppermute(value, "tp", pairs)

    def along_inner(value, j, way):
        pairs = [
            (o * inner + i, o * inner + way(i, j, inner))
            for o in range(outer)
            for i in range(inner)
        ]
        return lax.ppermute(value, "tp", pairs)

    columns = mod_weight.shape[1]
    copies = call(
        partial_body,
        sds((groups * ranks, 2, columns), BF16),
        cond_latent.reshape(1, -1),
        cond_context.reshape(1, -1),
        mod_weight,
        scratch=[
            pltpu.VMEM((2, cond_latent.shape[0]), F32),
            pltpu.VMEM(mod_weight.shape, BF16),
            pltpu.SemaphoreType.DMA((3,)),
        ],
        in_specs=[HBM] * 3,
        local=True,
    )
    pieces = lax.all_to_all(copies, ("sp", "tp"), 0, 0)

    blocks = {(0, 0): latent}
    for k in range(1, outer):
        if relayed(k):
            blocks[k, 0] = along_outer(blocks[k - 1, 0], 1, ahead)
        else:
            blocks[k, 0] = along_outer(latent, k, ahead)
    for j in range(1, inner):
        for k in range(outer):
            blocks[k, j] = along_inner(blocks[k, 0], j, ahead)

    here = (here_sp * ranks + here_tp).astype(jnp.int32).reshape(1)
    joined = wide + wide + VAL_DIM
    table, weight = call(
        functools.partial(table_body, number, pad, ranks, outer, inner),
        (sds((inner, 2, tile, wide), F32), sds((width, joined), BF16)),
        here,
        w_query,
        w_key,
        w_value,
        scratch=[pltpu.SemaphoreType.DMA((3,))],
        in_specs=[SMEM] + [HBM] * 3,
        local=True,
    )
    mod, q_first, kv_first = call(
        functools.partial(first_body, pad, ranks, outer),
        (
            sds((2, columns * ranks), F32),
            sds((tile, wide), BF16),
            sds((tile + held, wide + VAL_DIM), BF16),
        ),
        pieces,
        context,
        table,
        weight,
        *[blocks[k, 0] for k in range(outer)],
        scratch=[
            pltpu.VMEM((tile, width), BF16),
            pltpu.VMEM((held, width), BF16),
            pltpu.SemaphoreType.DMA,
        ],
        in_specs=[VMEM, HBM] + [VMEM] * (2 + outer),
    )
    queries, kv = [q_first], [kv_first]
    for j in range(1, inner):
        q_next, kv_next = call(
            functools.partial(second_body, pad, outer, j),
            (sds((tile, wide), BF16), sds((tile, wide + VAL_DIM), BF16)),
            mod,
            table,
            weight,
            *[blocks[k, j] for k in range(outer)],
            scratch=[pltpu.VMEM((tile, width), BF16)],
        )
        queries.append(q_next)
        kv.append(kv_next)
    share = share_of(groups)
    lines = groups // share

    def along_lines(value, s):
        pairs = [
            (g * share + c, ahead(g, s, lines) * share + c)
            for g in range(lines)
            for c in range(share)
        ]
        return lax.ppermute(value, "sp", pairs)

    swap = [(i, i ^ 1) for i in range(groups)]

    def spread(part):
        pieces = [part]
        for s in range(1, lines):
            pieces.append(along_lines(part, s))
        if share > 1:
            for piece in list(pieces):
                pieces.append(lax.ppermute(piece, "sp", swap))
        return pieces

    kv = [spread(part) for part in kv]
    early, late = kv[0], sum(kv[1:], [])
    stats = (
        sds((inner, 2, tile, 1), F32),
        sds((inner, 2, tile, 1), F32),
        sds((inner, 2, tile, VAL_DIM), F32),
    )

    def room(keys):
        return [
            pltpu.VMEM((inner, tile, wide), BF16),
            pltpu.VMEM((keys, wide), BF16),
            pltpu.VMEM((keys, VAL_DIM), BF16),
        ]

    keys = groups * (tile + held)
    first_stats = call(
        functools.partial(attend_first_body, number, pad, tile, inner),
        stats,
        *queries,
        *early,
        scratch=room(keys),
        extra=tile * keys * 12,
    )
    keys = groups * (inner - 1) * tile
    attended = call(
        functools.partial(attend_last_body, number, pad, tile, outer, inner),
        sds((outer, inner, pad, VAL_DIM), BF16),
        head_lambda,
        *first_stats,
        *queries,
        *late,
        scratch=room(keys),
        extra=tile * keys * 12,
        in_specs=[SMEM] + [VMEM] * (3 + inner + len(late)),
    )
    parts = [attended[0]]
    for k in range(1, outer):
        parts.append(along_outer(attended[k], k, behind))

    def joint(value, target):
        moves = []
        for s in range(groups):
            for o in range(outer):
                for i in range(inner):
                    to_s, to_o = target(s, o)
                    moves.append(
                        ((s * outer + o) * inner + i, (to_s * outer + to_o) * inner + i)
                    )
        return lax.ppermute(value, ("sp", "tp"), moves)

    slots, weights = [], []
    if share > 1 and outer == 4:
        fetched = joint(w_out, lambda s, o: (s, behind(o, 1 if s % 2 else 2, outer)))
        turned = joint(fetched, lambda s, o: (s ^ 1, o if s % 2 else behind(o, 1, outer)))
        given = jnp.where(here_sp % 2 == 0, fetched, turned)
        traded = lax.ppermute(given, "sp", swap)
        slots, weights = [(2, 1), (1, 3), (3, 2)], [fetched, turned, traded]
    else:
        for k in range(1, outer):
            weights.append(along_outer(w_out, k, behind))
            slots.append((k, k))
    depth = w_out.shape[0]
    total = call(
        functools.partial(partial_out_body, slots, share, ranks, inner, pad),
        (sds((pad, width), F32),) + (sds((pad, width), BF16),) * (inner - 1),
        here,
        w_out,
        *weights,
        *parts,
        scratch=[pltpu.VMEM((depth, width), BF16), pltpu.SemaphoreType.DMA],
        in_specs=[SMEM, HBM] + [VMEM] * (len(weights) + outer),
    )
    arrived = []
    for j in range(1, inner):
        arrived.append(along_inner(total[j], j, behind))
    return call(
        functools.partial(final_body, inner - 1),
        sds((number, width), BF16),
        latent,
        mod,
        total[0],
        *arrived,
    )


def relayed(k):
    return k > 1 and k % 2 == 1


def share_of(groups):
    return 2 if groups % 2 == 0 else 1


def solution(mesh):
    placed = (
        P(("sp", "tp"), None),
        P("sp", None),
        P("sp"),
        P("sp"),
        P("sp", "tp"),
        P(None, "tp"),
        P(None, "tp"),
        P(None, "tp"),
        P("tp", None),
        P("tp"),
    )
    return jax.shard_map(
        shards, mesh=mesh, in_specs=placed, out_specs=P(("sp", "tp"), None), check_vma=False
    )
```

```python
import functools

import jax
import jax.numpy as jnp
import numpy as np
from jax import lax
from jax.experimental import pallas as pl
from jax.experimental.pallas import tpu as pltpu
from jax.sharding import PartitionSpec as P

QK_DIM = 64
VAL_DIM = 128
GRID_W = 64

NORM_EPS = 0.01
HEAD_EPS = 0.001
THETA = 10000.0

F32 = jnp.float32
BF16 = jnp.bfloat16
VMEM = pl.BlockSpec(memory_space=pltpu.VMEM)
SMEM = pl.BlockSpec(memory_space=pltpu.SMEM)
NEAR = pl.BlockSpec(memory_space=pltpu.VMEM)
HBM = pl.BlockSpec(memory_space=pltpu.HBM)


def ahead(i, k, n):
    return i ^ k if n & (n - 1) == 0 else (i + k) % n


def behind(i, k, n):
    return i ^ k if n & (n - 1) == 0 else (i - k) % n


def split_of(size):
    inner = max(d for d in range(1, size + 1) if size % d == 0 and d * d <= size)
    return size // inner, inner


def size_of(v):
    return int(np.prod(v.shape)) * jnp.dtype(v.dtype).itemsize


def call(body, outs, *args, scratch=(), extra=0, local=False, flops=2000000, in_specs=None):
    held = sum(size_of(v) for v in args) + sum(size_of(v) for v in jax.tree.leaves(outs))
    held += sum(size_of(v) for v in scratch if hasattr(v, "dtype") and v.dtype in (F32, BF16))
    limit = min(60 * 1024 * 1024, held + extra + 6 * 1024 * 1024)
    in_specs = in_specs or [VMEM] * len(args)
    args = [
        pltpu.with_memory_space_constraint(v, pltpu.HBM)
        if spec is HBM
        else pltpu.with_memory_space_constraint(v, pltpu.VMEM)
        if spec is NEAR
        else v
        for v, spec in zip(args, in_specs)
    ]
    if local:
        outs = jax.tree.map(lambda v: pltpu.VMEM(v.shape, v.dtype), outs)
    return pl.pallas_call(
        body,
        out_shape=outs,
        in_specs=in_specs,
        out_specs=jax.tree.map(lambda _: VMEM, outs),
        scratch_shapes=list(scratch),
        compiler_params=pltpu.CompilerParams(vmem_limit_bytes=limit),
        cost_estimate=pl.CostEstimate(flops=flops, bytes_accessed=0, transcendentals=0),
    )(*args)


def sds(shape, dtype):
    return jax.ShapeDtypeStruct(shape, dtype)


def fetch_weights(sources, weight_ref, sems):
    moves, start = [], 0
    for i, source in enumerate(sources):
        columns = source.shape[1]
        moves.append(
            pltpu.make_async_copy(source, weight_ref.at[:, start : start + columns], sems.at[i])
        )
        moves[-1].start()
        start += columns
    return moves


def prepare_body(number, pad, ranks, outer, inner, *refs):
    here_ref, latent_hbm, context_hbm, weight_hbm = refs[:4]
    sources, exit_hbm = refs[4:7], refs[7]
    out_ref, table_ref, joined_ref, upper_ref, lower_ref = refs[8:13]
    cond_ref, weight_ref, sems, more_sems = refs[13:]
    half = upper_ref.shape[0]
    moves = [
        pltpu.make_async_copy(weight_hbm, weight_ref, sems.at[0]),
        pltpu.make_async_copy(latent_hbm, cond_ref.at[0:1], sems.at[1]),
        pltpu.make_async_copy(context_hbm, cond_ref.at[1:2], sems.at[2]),
    ]
    for move in moves:
        move.start()
    more = fetch_weights(sources, joined_ref, more_sems)
    more += [
        pltpu.make_async_copy(exit_hbm.at[:half], upper_ref, sems.at[3]),
        pltpu.make_async_copy(exit_hbm.at[half:], lower_ref, sems.at[4]),
    ]
    more[-2].start()
    more[-1].start()
    make_tables(number, pad, ranks, outer, inner, here_ref[0], table_ref)
    moves[1].wait()
    moves[2].wait()
    rows = cond_ref[...]
    rows = (rows / (1.0 + jnp.exp(-rows))).astype(BF16)
    moves[0].wait()
    part = jnp.dot(rows, weight_ref[...], preferred_element_type=F32).astype(BF16)
    for i in range(out_ref.shape[0]):
        out_ref[i] = part
    for move in more:
        move.wait()


def make_tables(number, pad, ranks, outer, inner, here, out_ref):
    group, rank = lax.div(here, ranks), lax.rem(here, ranks)
    here_outer, here_inner = lax.div(rank, inner), lax.rem(rank, inner)
    lane = lax.broadcasted_iota(jnp.int32, (pad, 2 * QK_DIM), 1)
    line = lax.broadcasted_iota(jnp.int32, (pad, 2 * QK_DIM), 0)
    low = lane < QK_DIM
    by_row = (lane & (QK_DIM - 1)) < QK_DIM // 2
    sign = jnp.where((lane & (QK_DIM // 4)) == 0, -1.0, 1.0)
    phase = jnp.where(low, np.float32(np.pi / 2), np.float32(0))
    shift = GRID_W.bit_length() - 1
    quarter = QK_DIM // 4
    inverse = jnp.ones(lane.shape, F32)
    for i in range(1, quarter):
        inverse = jnp.where((lane & (quarter - 1)) == i, np.float32(THETA ** (-i / quarter)), inverse)

    def owner(i, k, n):
        return i ^ k if n & (n - 1) == 0 else lax.rem(i + (n - k), n)

    for j in range(inner):
        for k in range(outer):
            rank_at = owner(here_outer, k, outer) * inner + owner(here_inner, j, inner)
            position = line + (group * ranks + rank_at) * number
            place = jnp.where(by_row, position >> shift, position & (GRID_W - 1)).astype(F32)
            wave = jnp.sin(place * inverse + phase)
            other = pltpu.roll(wave, QK_DIM, 1)
            out_ref[j, 0, k * pad : (k + 1) * pad, :] = jnp.where(low, wave, other)
            out_ref[j, 1, k * pad : (k + 1) * pad, :] = jnp.where(low, other, wave) * sign


def modulated(values, shift, scale):
    values = values.astype(F32)
    mean = jnp.mean(values * values, axis=-1, keepdims=True)
    return (values * lax.rsqrt(mean + NORM_EPS) * scale + shift).astype(BF16)


def fill_rows(blocks, rows_ref, pad, shift, scale):
    number = blocks[0].shape[0]
    for k, block in enumerate(blocks):
        rows_ref[k * pad : k * pad + number, :] = modulated(block[...], shift, scale)
        if pad > number:
            rows_ref[k * pad + number : (k + 1) * pad, :] = jnp.zeros(
                (pad - number, rows_ref.shape[1]), BF16
            )


def turn(u, cosine, sine):
    lane = lax.broadcasted_iota(jnp.int32, u.shape, 1)
    quarter = QK_DIM // 4
    width = u.shape[1]
    even = (lane // quarter) % 2 == 0
    turned = jnp.where(even, pltpu.roll(u, width - quarter, 1), pltpu.roll(u, quarter, 1))
    return (u * cosine + turned * sine).astype(BF16)


def context_body(ranks, *refs):
    pieces_ref, context_hbm, weight_ref, mod_ref, kv_ref, context_ref, sem = refs
    move = pltpu.make_async_copy(context_hbm, context_ref, sem)
    move.start()
    held, width = context_ref.shape
    columns = pieces_ref.shape[2]
    groups = pieces_ref.shape[0] // ranks
    for t in range(ranks):
        total = pieces_ref[t].astype(F32)
        for s in range(1, groups):
            total = total + pieces_ref[s * ranks + t].astype(F32)
        mod_ref[:, t * columns : (t + 1) * columns] = total
    shift, scale = mod_ref[1:2, :width], 1.0 + mod_ref[1:2, width : 2 * width]
    step = 16 if held % 16 == 0 else held
    move.wait()
    for i in range(0, held, step):
        context_ref[i : i + step, :] = modulated(context_ref[i : i + step, :], shift, scale)
    kv_ref[...] = jnp.dot(
        context_ref[...], weight_ref[:, 2 * QK_DIM :], preferred_element_type=F32
    ).astype(BF16)


def rows_body(pad, outer, inner, *refs):
    mod_ref, table_ref, weight_ref = refs[:3]
    blocks = refs[3:-3]
    q_ref, kv_ref, rows_ref = refs[-3:]
    width = blocks[0].shape[1]
    fill_rows(
        blocks, rows_ref, pad, mod_ref[0:1, :width], 1.0 + mod_ref[0:1, width : 2 * width]
    )
    tile, wide = outer * pad, 2 * QK_DIM
    product = jnp.dot(rows_ref[...], weight_ref[...], preferred_element_type=F32)
    for j in range(inner):
        u = product[j * tile : (j + 1) * tile]
        cosine, sine = table_ref[j, 0], table_ref[j, 1]
        scale = jnp.asarray(QK_DIM ** (-0.5), BF16)
        q_ref[j] = turn(u[:, :wide], cosine, sine) * scale
        kv_ref[j * tile : (j + 1) * tile, :wide] = turn(u[:, wide : 2 * wide], cosine, sine)
        kv_ref[j * tile : (j + 1) * tile, wide:] = u[:, 2 * wide :].astype(BF16)


def gather_pieces(pieces, padded, number, pad, k_all, v_all):
    wide = 2 * QK_DIM
    row = latents = 0
    for i, piece in enumerate(pieces):
        rows = piece.shape[0]
        k_all[row : row + rows, :] = piece[:, :wide]
        v_all[row : row + rows, :] = piece[:, wide:]
        row += rows
        latents += rows if i < padded else 0
    column = lax.broadcasted_iota(jnp.int32, (1, row), 1)
    valid = (column >= latents) | (column % pad < number)
    return jnp.where(valid, 0.0, -1e30)


def score(q_ref, j, m, k_all):
    queries = q_ref[j]
    lane = lax.broadcasted_iota(jnp.int32, queries.shape, 1)
    own = jnp.where((lane // QK_DIM) == m, queries, jnp.zeros_like(queries))
    return lax.dot_general(
        own, k_all[...], (((1,), (1,)), ((), ())), preferred_element_type=F32
    )


def repeat(count, one):
    if count <= 4:
        for j in range(count):
            one(j, 0)
    else:
        lax.fori_loop(0, count, one, 0)


def attend_first_body(number, pad, padded, inner, *refs):
    q_ref, kv_refs = refs[0], refs[1:-5]
    top_ref, sum_ref, mix_ref, k_all, v_all = refs[-5:]
    bias = gather_pieces(kv_refs, padded, number, pad, k_all, v_all)

    def one(j, carry):
        for m in range(2):
            scores = score(q_ref, j, m, k_all) + bias
            highest = jnp.max(scores, axis=-1, keepdims=True)
            weights = jnp.exp(scores - highest)
            top_ref[j, m] = highest
            sum_ref[j, m] = jnp.sum(weights, axis=-1, keepdims=True)
            mix_ref[j, m] = jnp.dot(
                weights.astype(BF16), v_all[...], preferred_element_type=F32
            )
        return carry

    repeat(inner, one)


def attend_last_body(number, pad, outer, inner, *refs):
    factor_ref, top_ref, sum_ref, mix_ref, q_ref = refs[:5]
    kv_refs, (out_ref, k_all, v_all) = refs[5:-3], refs[-3:]
    bias = gather_pieces(kv_refs, len(kv_refs), number, pad, k_all, v_all)

    def one(j, carry):
        mixed = []
        for m in range(2):
            scores = score(q_ref, j, m, k_all) + bias
            before = top_ref[j, m]
            highest = jnp.maximum(before, jnp.max(scores, axis=-1, keepdims=True))
            fade = jnp.exp(before - highest)
            weights = jnp.exp(scores - highest)
            totals = sum_ref[j, m] * fade + jnp.sum(weights, axis=-1, keepdims=True)
            mix = mix_ref[j, m] * fade + jnp.dot(
                weights.astype(BF16), v_all[...], preferred_element_type=F32
            )
            mixed.append(mix / totals)
        head = mixed[0] - factor_ref[0] * mixed[1]
        head = head * lax.rsqrt(jnp.mean(head * head, axis=-1, keepdims=True) + HEAD_EPS)
        head = head.astype(BF16)
        for k in range(outer):
            out_ref[k, j] = head[k * pad : (k + 1) * pad]
        return carry

    repeat(inner, one)


def partial_out_body(slots, share, ranks, outer, inner, pad, *refs):
    here_ref, own_hbm = refs[:2]
    held = refs[2 : 2 + len(slots)]
    rest = refs[2 + len(slots) : -2]
    own_weight, sem = refs[-2:]
    move = pltpu.make_async_copy(own_hbm, own_weight, sem)
    move.start()
    parts, own_ref, others = rest[:outer], rest[outer], rest[1 + outer :]
    rows = inner * pad
    side = lax.rem(lax.div(here_ref[0], ranks), share)
    first = jnp.broadcast_to(side, (rows, VAL_DIM)) == 0

    def part(k):
        return parts[k][...].reshape(rows, VAL_DIM)

    total, start = None, 0
    for (a, b), weight in zip(slots, held):
        rows_in = part(a) if a == b else jnp.where(first, part(a), part(b))
        rows_in = rows_in[:, start : start + weight.shape[0]]
        start = (start + weight.shape[0]) % VAL_DIM
        term = jnp.dot(rows_in, weight[...], preferred_element_type=F32)
        total = term if total is None else total + term
    move.wait()
    total += jnp.dot(part(0), own_weight[...], preferred_element_type=F32)
    own_ref[...] = total[:pad]
    for j in range(1, inner):
        others[j - 1][...] = total[j * pad : (j + 1) * pad].astype(BF16)


def final_body(count, *refs):
    latent_ref, mod_ref, own_ref = refs[:3]
    others = refs[3 : 3 + count]
    out_ref = refs[3 + count]
    number, width = out_ref.shape
    total = own_ref[...]
    for other in others:
        total = total + other[...].astype(F32)
    total = total[:number]
    total = total * lax.rsqrt(jnp.mean(total * total, axis=-1, keepdims=True) + NORM_EPS)
    gate = mod_ref[0:1, 2 * width :]
    out_ref[...] = (latent_ref[...].astype(F32) + gate * total).astype(BF16)


def shards(
    latent,
    context,
    cond_latent,
    cond_context,
    mod_weight,
    w_query,
    w_key,
    w_value,
    w_out,
    head_lambda,
):
    number, width = latent.shape
    groups, ranks = lax.axis_size("sp"), lax.axis_size("tp")
    outer, inner = split_of(ranks)
    pad = -(-number // 16) * 16
    wide = 2 * QK_DIM
    tile = outer * pad
    held = context.shape[0]
    here_sp, here_tp = lax.axis_index("sp"), lax.axis_index("tp")

    def along_outer(value, k, way):
        pairs = [
            (o * inner + i, way(o, k, outer) * inner + i)
            for o in range(outer)
            for i in range(inner)
        ]
        return lax.ppermute(value, "tp", pairs)

    def along_inner(value, j, way):
        pairs = [
            (o * inner + i, o * inner + way(i, j, inner))
            for o in range(outer)
            for i in range(inner)
        ]
        return lax.ppermute(value, "tp", pairs)

    columns = mod_weight.shape[1]
    here = (here_sp * ranks + here_tp).astype(jnp.int32).reshape(1)
    depth = w_out.shape[0]
    half = sds((depth // 2, width), BF16)
    copies, table, weight, *halves = call(
        functools.partial(prepare_body, number, pad, ranks, outer, inner),
        (
            sds((groups * ranks, 2, columns), BF16),
            sds((inner, 2, tile, wide), F32),
            sds((width, wide + wide + VAL_DIM), BF16),
            half,
            half,
        ),
        here,
        cond_latent.reshape(1, -1),
        cond_context.reshape(1, -1),
        mod_weight,
        w_query,
        w_key,
        w_value,
        w_out,
        scratch=[
            pltpu.VMEM((2, cond_latent.shape[0]), F32),
            pltpu.VMEM(mod_weight.shape, BF16),
            pltpu.SemaphoreType.DMA((5,)),
            pltpu.SemaphoreType.DMA((3,)),
        ],
        in_specs=[SMEM] + [HBM] * 7,
        local=True,
    )
    pieces = lax.all_to_all(copies, ("sp", "tp"), 0, 0)

    blocks = {(0, 0): latent}
    for k in range(1, outer):
        if relayed(k):
            blocks[k, 0] = along_outer(blocks[k - 1, 0], 1, ahead)
        else:
            blocks[k, 0] = along_outer(latent, k, ahead)
    for j in range(1, inner):
        for k in range(outer):
            blocks[k, j] = along_inner(blocks[k, 0], j, ahead)

    mod, kv_context = call(
        functools.partial(context_body, ranks),
        (sds((2, columns * ranks), F32), sds((held, wide + VAL_DIM), BF16)),
        pieces,
        context,
        weight,
        scratch=[pltpu.VMEM((held, width), BF16), pltpu.SemaphoreType.DMA],
        in_specs=[VMEM, HBM, VMEM],
        local=True,
    )
    queries, kv = call(
        functools.partial(rows_body, pad, outer, inner),
        (sds((inner, tile, wide), BF16), sds((inner * tile, wide + VAL_DIM), BF16)),
        mod,
        table,
        weight,
        *[blocks[k, j] for j in range(inner) for k in range(outer)],
        scratch=[pltpu.VMEM((inner * tile, width), BF16)],
        extra=inner * tile * 6 * QK_DIM * 4,
        local=True,
    )
    share = share_of(groups)
    lines = groups // share

    def along_lines(value, s):
        pairs = [
            (g * share + c, ahead(g, s, lines) * share + c)
            for g in range(lines)
            for c in range(share)
        ]
        return lax.ppermute(value, "sp", pairs)

    swap = [(i, i ^ 1) for i in range(groups)]

    def spread(part):
        pieces = [part]
        for s in range(1, lines):
            pieces.append(along_lines(part, s))
        if share > 1:
            for piece in list(pieces):
                pieces.append(lax.ppermute(piece, "sp", swap))
        return pieces

    near, late = spread(kv_context), spread(kv)
    first = [i for i in range(len(late)) if i % lines == 0]
    early = [late[i] for i in first] + near
    late = [v for i, v in enumerate(late) if i not in first]
    stats = (
        sds((inner, 2, tile, 1), F32),
        sds((inner, 2, tile, 1), F32),
        sds((inner, 2, tile, VAL_DIM), F32),
    )

    def room(keys):
        return [pltpu.VMEM((keys, wide), BF16), pltpu.VMEM((keys, VAL_DIM), BF16)]

    keys = groups * held + len(first) * inner * tile
    first_stats = call(
        functools.partial(attend_first_body, number, pad, len(first), inner),
        stats,
        queries,
        *early,
        scratch=room(keys),
        extra=tile * keys * 12,
        local=True,
    )
    keys = len(late) * inner * tile
    attended = call(
        functools.partial(attend_last_body, number, pad, outer, inner),
        sds((outer, inner, pad, VAL_DIM), BF16),
        head_lambda,
        *first_stats,
        queries,
        *late,
        scratch=room(keys),
        extra=tile * keys * 12,
        in_specs=[SMEM] + [VMEM] * (4 + len(late)),
        local=True,
    )
    parts = [attended[0]]
    for k in range(1, outer):
        parts.append(along_outer(attended[k], k, behind))

    def joint(value, target):
        moves = []
        for s in range(groups):
            for o in range(outer):
                for i in range(inner):
                    to_s, to_o = target(s, o)
                    moves.append(
                        ((s * outer + o) * inner + i, (to_s * outer + to_o) * inner + i)
                    )
        return lax.ppermute(value, ("sp", "tp"), moves)

    slots, weights = [], []
    if share > 1 and outer == 4:
        fetched, turned = [], []
        for i, part in enumerate(halves):
            fetched.append(
                joint(part, lambda s, o: (s, behind(o, 1 if s % 2 else 2, outer)))
            )
            turned.append(
                joint(fetched[i], lambda s, o: (s ^ 1, o if s % 2 else behind(o, 1, outer)))
            )
        given = [jnp.where(here_sp % 2 == 0, a, b) for a, b in zip(fetched, turned)]
        traded = lax.ppermute(jnp.concatenate(given, axis=0), "sp", swap)
        slots = [(2, 1), (2, 1), (1, 3), (1, 3), (3, 2)]
        weights = [*fetched, *turned, traded]
    else:
        for k in range(1, outer):
            weights.append(along_outer(w_out, k, behind))
            slots.append((k, k))
    total = call(
        functools.partial(partial_out_body, slots, share, ranks, outer, inner, pad),
        (sds((pad, width), F32),) + (sds((pad, width), BF16),) * (inner - 1),
        here,
        w_out,
        *weights,
        *parts,
        scratch=[pltpu.VMEM((depth, width), BF16), pltpu.SemaphoreType.DMA],
        in_specs=[SMEM, HBM] + [VMEM] * (len(weights) + outer),
    )
    arrived = []
    for j in range(1, inner):
        arrived.append(along_inner(total[j], j, behind))
    return call(
        functools.partial(final_body, inner - 1),
        sds((number, width), BF16),
        latent,
        mod,
        total[0],
        *arrived,
    )


def relayed(k):
    return k > 1 and k % 2 == 1


def share_of(groups):
    return 2 if groups % 2 == 0 else 1


def solution(mesh):
    placed = (
        P(("sp", "tp"), None),
        P("sp", None),
        P("sp"),
        P("sp"),
        P("sp", "tp"),
        P(None, "tp"),
        P(None, "tp"),
        P(None, "tp"),
        P("tp", None),
        P("tp"),
    )
    return jax.shard_map(
        shards, mesh=mesh, in_specs=placed, out_specs=P(("sp", "tp"), None), check_vma=False
    )
```

```python
import functools

import jax
import jax.numpy as jnp
import numpy as np
from jax import lax
from jax.experimental import pallas as pl
from jax.experimental.pallas import tpu as pltpu
from jax.sharding import PartitionSpec as P

QK_DIM = 64
VAL_DIM = 128
GRID_W = 64

NORM_EPS = 0.01
HEAD_EPS = 0.001
THETA = 10000.0

F32 = jnp.float32
BF16 = jnp.bfloat16
VMEM = pl.BlockSpec(memory_space=pltpu.VMEM)
SMEM = pl.BlockSpec(memory_space=pltpu.SMEM)
NEAR = pl.BlockSpec(memory_space=pltpu.VMEM)
HBM = pl.BlockSpec(memory_space=pltpu.HBM)


def ahead(i, k, n):
    return i ^ k if n & (n - 1) == 0 else (i + k) % n


def behind(i, k, n):
    return i ^ k if n & (n - 1) == 0 else (i - k) % n


def split_of(size):
    inner = max(d for d in range(1, size + 1) if size % d == 0 and d * d <= size)
    return size // inner, inner


def size_of(v):
    return int(np.prod(v.shape)) * jnp.dtype(v.dtype).itemsize


def call(body, outs, *args, scratch=(), extra=0, local=False, flops=2000000, in_specs=None):
    held = sum(size_of(v) for v in args) + sum(size_of(v) for v in jax.tree.leaves(outs))
    held += sum(size_of(v) for v in scratch if hasattr(v, "dtype") and v.dtype in (F32, BF16))
    limit = min(60 * 1024 * 1024, held + extra + 6 * 1024 * 1024)
    in_specs = in_specs or [VMEM] * len(args)
    args = [
        pltpu.with_memory_space_constraint(v, pltpu.HBM)
        if spec is HBM
        else pltpu.with_memory_space_constraint(v, pltpu.VMEM)
        if spec is NEAR
        else v
        for v, spec in zip(args, in_specs)
    ]
    if local:
        outs = jax.tree.map(lambda v: pltpu.VMEM(v.shape, v.dtype), outs)
    return pl.pallas_call(
        body,
        out_shape=outs,
        in_specs=in_specs,
        out_specs=jax.tree.map(lambda _: VMEM, outs),
        scratch_shapes=list(scratch),
        compiler_params=pltpu.CompilerParams(vmem_limit_bytes=limit),
        cost_estimate=pl.CostEstimate(flops=flops, bytes_accessed=0, transcendentals=0),
    )(*args)


def sds(shape, dtype):
    return jax.ShapeDtypeStruct(shape, dtype)


def fetch_weights(sources, weight_ref, sems):
    moves, start = [], 0
    for i, source in enumerate(sources):
        columns = source.shape[1]
        moves.append(
            pltpu.make_async_copy(source, weight_ref.at[:, start : start + columns], sems.at[i])
        )
        moves[-1].start()
        start += columns
    return moves


def prepare_body(number, pad, ranks, outer, inner, *refs):
    here_ref, latent_hbm, context_hbm, weight_hbm = refs[:4]
    sources = refs[4:7]
    out_ref, table_ref, joined_ref, cond_ref, weight_ref, sems, more_sems = refs[7:]
    moves = [
        pltpu.make_async_copy(weight_hbm, weight_ref, sems.at[0]),
        pltpu.make_async_copy(latent_hbm, cond_ref.at[0:1], sems.at[1]),
        pltpu.make_async_copy(context_hbm, cond_ref.at[1:2], sems.at[2]),
    ]
    for move in moves:
        move.start()
    more = fetch_weights(sources, joined_ref, more_sems)
    make_tables(number, pad, ranks, outer, inner, here_ref[0], table_ref)
    moves[1].wait()
    moves[2].wait()
    rows = cond_ref[...]
    rows = (rows / (1.0 + jnp.exp(-rows))).astype(BF16)
    moves[0].wait()
    part = jnp.dot(rows, weight_ref[...], preferred_element_type=F32).astype(BF16)
    for i in range(out_ref.shape[0]):
        out_ref[i] = part
    for move in more:
        move.wait()


def make_tables(number, pad, ranks, outer, inner, here, out_ref):
    group, rank = lax.div(here, ranks), lax.rem(here, ranks)
    here_outer, here_inner = lax.div(rank, inner), lax.rem(rank, inner)
    lane = lax.broadcasted_iota(jnp.int32, (pad, 2 * QK_DIM), 1)
    line = lax.broadcasted_iota(jnp.int32, (pad, 2 * QK_DIM), 0)
    low = lane < QK_DIM
    by_row = (lane & (QK_DIM - 1)) < QK_DIM // 2
    sign = jnp.where((lane & (QK_DIM // 4)) == 0, -1.0, 1.0)
    phase = jnp.where(low, np.float32(np.pi / 2), np.float32(0))
    shift = GRID_W.bit_length() - 1
    quarter = QK_DIM // 4
    inverse = jnp.ones(lane.shape, F32)
    for i in range(1, quarter):
        inverse = jnp.where((lane & (quarter - 1)) == i, np.float32(THETA ** (-i / quarter)), inverse)

    def owner(i, k, n):
        return i ^ k if n & (n - 1) == 0 else lax.rem(i + (n - k), n)

    for j in range(inner):
        for k in range(outer):
            rank_at = owner(here_outer, k, outer) * inner + owner(here_inner, j, inner)
            position = line + (group * ranks + rank_at) * number
            place = jnp.where(by_row, position >> shift, position & (GRID_W - 1)).astype(F32)
            wave = jnp.sin(place * inverse + phase)
            other = pltpu.roll(wave, QK_DIM, 1)
            out_ref[j, 0, k * pad : (k + 1) * pad, :] = jnp.where(low, wave, other)
            out_ref[j, 1, k * pad : (k + 1) * pad, :] = jnp.where(low, other, wave) * sign


def modulated(values, shift, scale):
    values = values.astype(F32)
    mean = jnp.mean(values * values, axis=-1, keepdims=True)
    return (values * lax.rsqrt(mean + NORM_EPS) * scale + shift).astype(BF16)


def fill_rows(blocks, rows_ref, pad, shift, scale):
    number = blocks[0].shape[0]
    for k, block in enumerate(blocks):
        rows_ref[k * pad : k * pad + number, :] = modulated(block[...], shift, scale)
        if pad > number:
            rows_ref[k * pad + number : (k + 1) * pad, :] = jnp.zeros(
                (pad - number, rows_ref.shape[1]), BF16
            )


def turn(u, cosine, sine):
    lane = lax.broadcasted_iota(jnp.int32, u.shape, 1)
    quarter = QK_DIM // 4
    width = u.shape[1]
    even = (lane // quarter) % 2 == 0
    turned = jnp.where(even, pltpu.roll(u, width - quarter, 1), pltpu.roll(u, quarter, 1))
    return (u * cosine + turned * sine).astype(BF16)


def context_body(ranks, *refs):
    pieces_ref, context_hbm, weight_ref, mod_ref, kv_ref, context_ref, sem = refs
    move = pltpu.make_async_copy(context_hbm, context_ref, sem)
    move.start()
    held, width = context_ref.shape
    columns = pieces_ref.shape[2]
    groups = pieces_ref.shape[0] // ranks
    for t in range(ranks):
        total = pieces_ref[t].astype(F32)
        for s in range(1, groups):
            total = total + pieces_ref[s * ranks + t].astype(F32)
        mod_ref[:, t * columns : (t + 1) * columns] = total
    shift, scale = mod_ref[1:2, :width], 1.0 + mod_ref[1:2, width : 2 * width]
    step = 16 if held % 16 == 0 else held
    move.wait()
    for i in range(0, held, step):
        context_ref[i : i + step, :] = modulated(context_ref[i : i + step, :], shift, scale)
    kv_ref[...] = jnp.dot(
        context_ref[...], weight_ref[:, 2 * QK_DIM :], preferred_element_type=F32
    ).astype(BF16)


def rows_body(pad, outer, inner, *refs):
    mod_ref, table_ref, weight_ref = refs[:3]
    blocks = refs[3:-3]
    q_ref, kv_ref, rows_ref = refs[-3:]
    width = blocks[0].shape[1]
    fill_rows(
        blocks, rows_ref, pad, mod_ref[0:1, :width], 1.0 + mod_ref[0:1, width : 2 * width]
    )
    tile, wide = outer * pad, 2 * QK_DIM
    product = jnp.dot(rows_ref[...], weight_ref[...], preferred_element_type=F32)
    for j in range(inner):
        u = product[j * tile : (j + 1) * tile]
        cosine, sine = table_ref[j, 0], table_ref[j, 1]
        scale = jnp.asarray(QK_DIM ** (-0.5), BF16)
        q_ref[j] = turn(u[:, :wide], cosine, sine) * scale
        kv_ref[j * tile : (j + 1) * tile, :wide] = turn(u[:, wide : 2 * wide], cosine, sine)
        kv_ref[j * tile : (j + 1) * tile, wide:] = u[:, 2 * wide :].astype(BF16)


def gather_pieces(pieces, padded, number, pad, k_all, v_all):
    wide = 2 * QK_DIM
    row = latents = 0
    for i, piece in enumerate(pieces):
        rows = piece.shape[0]
        k_all[row : row + rows, :] = piece[:, :wide]
        v_all[row : row + rows, :] = piece[:, wide:]
        row += rows
        latents += rows if i < padded else 0
    column = lax.broadcasted_iota(jnp.int32, (1, row), 1)
    valid = (column >= latents) | (column % pad < number)
    return jnp.where(valid, 0.0, -1e30)


def score(q_ref, j, m, k_all):
    queries = q_ref[j]
    lane = lax.broadcasted_iota(jnp.int32, queries.shape, 1)
    own = jnp.where((lane // QK_DIM) == m, queries, jnp.zeros_like(queries))
    return lax.dot_general(
        own, k_all[...], (((1,), (1,)), ((), ())), preferred_element_type=F32
    )


def repeat(count, one):
    if count <= 4:
        for j in range(count):
            one(j, 0)
    else:
        lax.fori_loop(0, count, one, 0)


def attend_first_body(number, pad, padded, inner, *refs):
    q_ref, kv_refs = refs[0], refs[1:-5]
    top_ref, sum_ref, mix_ref, k_all, v_all = refs[-5:]
    bias = gather_pieces(kv_refs, padded, number, pad, k_all, v_all)

    def one(j, carry):
        for m in range(2):
            scores = score(q_ref, j, m, k_all) + bias
            highest = jnp.max(scores, axis=-1, keepdims=True)
            weights = jnp.exp(scores - highest)
            top_ref[j, m] = highest
            sum_ref[j, m] = jnp.sum(weights, axis=-1, keepdims=True)
            mix_ref[j, m] = jnp.dot(
                weights.astype(BF16), v_all[...], preferred_element_type=F32
            )
        return carry

    repeat(inner, one)


def attend_last_body(number, pad, outer, inner, *refs):
    factor_ref, top_ref, sum_ref, mix_ref, q_ref = refs[:5]
    kv_refs, (out_ref, k_all, v_all) = refs[5:-3], refs[-3:]
    bias = gather_pieces(kv_refs, len(kv_refs), number, pad, k_all, v_all)

    def one(j, carry):
        mixed = []
        for m in range(2):
            scores = score(q_ref, j, m, k_all) + bias
            before = top_ref[j, m]
            highest = jnp.maximum(before, jnp.max(scores, axis=-1, keepdims=True))
            fade = jnp.exp(before - highest)
            weights = jnp.exp(scores - highest)
            totals = sum_ref[j, m] * fade + jnp.sum(weights, axis=-1, keepdims=True)
            mix = mix_ref[j, m] * fade + jnp.dot(
                weights.astype(BF16), v_all[...], preferred_element_type=F32
            )
            mixed.append(mix / totals)
        head = mixed[0] - factor_ref[0] * mixed[1]
        head = head * lax.rsqrt(jnp.mean(head * head, axis=-1, keepdims=True) + HEAD_EPS)
        head = head.astype(BF16)
        for k in range(outer):
            out_ref[k, j] = head[k * pad : (k + 1) * pad]
        return carry

    repeat(inner, one)


def partial_out_body(slots, share, ranks, outer, inner, pad, *refs):
    here_ref, own_hbm = refs[:2]
    held = refs[2 : 2 + len(slots)]
    rest = refs[2 + len(slots) : -2]
    own_weight, sem = refs[-2:]
    move = pltpu.make_async_copy(own_hbm, own_weight, sem)
    move.start()
    parts, own_ref, others = rest[:outer], rest[outer], rest[1 + outer :]
    rows = inner * pad
    side = lax.rem(lax.div(here_ref[0], ranks), share)
    first = jnp.broadcast_to(side, (rows, VAL_DIM)) == 0

    def part(k):
        return parts[k][...].reshape(rows, VAL_DIM)

    total, start = None, 0
    for (a, b), weight in zip(slots, held):
        rows_in = part(a) if a == b else jnp.where(first, part(a), part(b))
        rows_in = rows_in[:, start : start + weight.shape[0]]
        start = (start + weight.shape[0]) % VAL_DIM
        term = jnp.dot(rows_in, weight[...], preferred_element_type=F32)
        total = term if total is None else total + term
    move.wait()
    total += jnp.dot(part(0), own_weight[...], preferred_element_type=F32)
    own_ref[...] = total[:pad]
    for j in range(1, inner):
        others[j - 1][...] = total[j * pad : (j + 1) * pad].astype(BF16)


def final_body(count, *refs):
    latent_ref, mod_ref, own_ref = refs[:3]
    others = refs[3 : 3 + count]
    out_ref = refs[3 + count]
    number, width = out_ref.shape
    total = own_ref[...]
    for other in others:
        total = total + other[...].astype(F32)
    total = total[:number]
    total = total * lax.rsqrt(jnp.mean(total * total, axis=-1, keepdims=True) + NORM_EPS)
    gate = mod_ref[0:1, 2 * width :]
    out_ref[...] = (latent_ref[...].astype(F32) + gate * total).astype(BF16)


def shards(
    latent,
    context,
    cond_latent,
    cond_context,
    mod_weight,
    w_query,
    w_key,
    w_value,
    w_out,
    head_lambda,
):
    number, width = latent.shape
    groups, ranks = lax.axis_size("sp"), lax.axis_size("tp")
    outer, inner = split_of(ranks)
    pad = -(-number // 16) * 16
    wide = 2 * QK_DIM
    tile = outer * pad
    held = context.shape[0]
    here_sp, here_tp = lax.axis_index("sp"), lax.axis_index("tp")

    def along_outer(value, k, way):
        pairs = [
            (o * inner + i, way(o, k, outer) * inner + i)
            for o in range(outer)
            for i in range(inner)
        ]
        return lax.ppermute(value, "tp", pairs)

    def along_inner(value, j, way):
        pairs = [
            (o * inner + i, o * inner + way(i, j, inner))
            for o in range(outer)
            for i in range(inner)
        ]
        return lax.ppermute(value, "tp", pairs)

    columns = mod_weight.shape[1]
    here = (here_sp * ranks + here_tp).astype(jnp.int32).reshape(1)
    copies, table, weight = call(
        functools.partial(prepare_body, number, pad, ranks, outer, inner),
        (
            sds((groups * ranks, 2, columns), BF16),
            sds((inner, 2, tile, wide), F32),
            sds((width, wide + wide + VAL_DIM), BF16),
        ),
        here,
        cond_latent.reshape(1, -1),
        cond_context.reshape(1, -1),
        mod_weight,
        w_query,
        w_key,
        w_value,
        scratch=[
            pltpu.VMEM((2, cond_latent.shape[0]), F32),
            pltpu.VMEM(mod_weight.shape, BF16),
            pltpu.SemaphoreType.DMA((3,)),
            pltpu.SemaphoreType.DMA((3,)),
        ],
        in_specs=[SMEM] + [HBM] * 6,
        local=True,
    )
    pieces = lax.all_to_all(copies, ("sp", "tp"), 0, 0)

    blocks = {(0, 0): latent}
    for k in range(1, outer):
        if relayed(k):
            blocks[k, 0] = along_outer(blocks[k - 1, 0], 1, ahead)
        else:
            blocks[k, 0] = along_outer(latent, k, ahead)
    for j in range(1, inner):
        for k in range(outer):
            blocks[k, j] = along_inner(blocks[k, 0], j, ahead)

    mod, kv_context = call(
        functools.partial(context_body, ranks),
        (sds((2, columns * ranks), F32), sds((held, wide + VAL_DIM), BF16)),
        pieces,
        context,
        weight,
        scratch=[pltpu.VMEM((held, width), BF16), pltpu.SemaphoreType.DMA],
        in_specs=[VMEM, HBM, VMEM],
        local=True,
    )
    queries, kv = call(
        functools.partial(rows_body, pad, outer, inner),
        (sds((inner, tile, wide), BF16), sds((inner * tile, wide + VAL_DIM), BF16)),
        mod,
        table,
        weight,
        *[blocks[k, j] for j in range(inner) for k in range(outer)],
        scratch=[pltpu.VMEM((inner * tile, width), BF16)],
        extra=inner * tile * 6 * QK_DIM * 4,
        local=True,
    )
    share = share_of(groups)
    lines = groups // share

    def along_lines(value, s):
        pairs = [
            (g * share + c, ahead(g, s, lines) * share + c)
            for g in range(lines)
            for c in range(share)
        ]
        return lax.ppermute(value, "sp", pairs)

    swap = [(i, i ^ 1) for i in range(groups)]

    def spread(part):
        pieces = [part]
        for s in range(1, lines):
            pieces.append(along_lines(part, s))
        if share > 1:
            for piece in list(pieces):
                pieces.append(lax.ppermute(piece, "sp", swap))
        return pieces

    near, late = spread(kv_context), spread(kv)
    first = [i for i in range(len(late)) if i % lines == 0]
    early = [late[i] for i in first] + near
    late = [v for i, v in enumerate(late) if i not in first]
    stats = (
        sds((inner, 2, tile, 1), F32),
        sds((inner, 2, tile, 1), F32),
        sds((inner, 2, tile, VAL_DIM), F32),
    )

    def room(keys):
        return [pltpu.VMEM((keys, wide), BF16), pltpu.VMEM((keys, VAL_DIM), BF16)]

    keys = groups * held + len(first) * inner * tile
    first_stats = call(
        functools.partial(attend_first_body, number, pad, len(first), inner),
        stats,
        queries,
        *early,
        scratch=room(keys),
        extra=tile * keys * 12,
        local=True,
    )
    keys = len(late) * inner * tile
    attended = call(
        functools.partial(attend_last_body, number, pad, outer, inner),
        sds((outer, inner, pad, VAL_DIM), BF16),
        head_lambda,
        *first_stats,
        queries,
        *late,
        scratch=room(keys),
        extra=tile * keys * 12,
        in_specs=[SMEM] + [VMEM] * (4 + len(late)),
        local=True,
    )
    parts = [attended[0]]
    for k in range(1, outer):
        parts.append(along_outer(attended[k], k, behind))

    def joint(value, target):
        moves = []
        for s in range(groups):
            for o in range(outer):
                for i in range(inner):
                    to_s, to_o = target(s, o)
                    moves.append(
                        ((s * outer + o) * inner + i, (to_s * outer + to_o) * inner + i)
                    )
        return lax.ppermute(value, ("sp", "tp"), moves)

    slots, weights = [], []
    if share > 1 and outer == 4:
        fetched = joint(w_out, lambda s, o: (s, behind(o, 1 if s % 2 else 2, outer)))
        turned = joint(fetched, lambda s, o: (s ^ 1, o if s % 2 else behind(o, 1, outer)))
        given = jnp.where(here_sp % 2 == 0, fetched, turned)
        traded = lax.ppermute(given, "sp", swap)
        slots, weights = [(2, 1), (1, 3), (3, 2)], [fetched, turned, traded]
    else:
        for k in range(1, outer):
            weights.append(along_outer(w_out, k, behind))
            slots.append((k, k))
    depth = w_out.shape[0]
    total = call(
        functools.partial(partial_out_body, slots, share, ranks, outer, inner, pad),
        (sds((pad, width), F32),) + (sds((pad, width), BF16),) * (inner - 1),
        here,
        w_out,
        *weights,
        *parts,
        scratch=[pltpu.VMEM((depth, width), BF16), pltpu.SemaphoreType.DMA],
        in_specs=[SMEM, HBM] + [VMEM] * (len(weights) + outer),
    )
    arrived = []
    for j in range(1, inner):
        arrived.append(along_inner(total[j], j, behind))
    return call(
        functools.partial(final_body, inner - 1),
        sds((number, width), BF16),
        latent,
        mod,
        total[0],
        *arrived,
    )


def relayed(k):
    return k > 1 and k % 2 == 1


def share_of(groups):
    return 2 if groups % 2 == 0 else 1


def solution(mesh):
    placed = (
        P(("sp", "tp"), None),
        P("sp", None),
        P("sp"),
        P("sp"),
        P("sp", "tp"),
        P(None, "tp"),
        P(None, "tp"),
        P(None, "tp"),
        P("tp", None),
        P("tp"),
    )
    return jax.shard_map(
        shards, mesh=mesh, in_specs=placed, out_specs=P(("sp", "tp"), None), check_vma=False
    )
```

```python
import functools

import jax
import jax.numpy as jnp
import numpy as np
from jax import lax
from jax.experimental import pallas as pl
from jax.experimental.pallas import tpu as pltpu
from jax.sharding import PartitionSpec as P

QK_DIM = 64
VAL_DIM = 128
GRID_W = 64

NORM_EPS = 0.01
HEAD_EPS = 0.001
THETA = 10000.0

F32 = jnp.float32
BF16 = jnp.bfloat16
VMEM = pl.BlockSpec(memory_space=pltpu.VMEM)
SMEM = pl.BlockSpec(memory_space=pltpu.SMEM)
NEAR = pl.BlockSpec(memory_space=pltpu.VMEM)
HBM = pl.BlockSpec(memory_space=pltpu.HBM)


def ahead(i, k, n):
    return i ^ k if n & (n - 1) == 0 else (i + k) % n


def behind(i, k, n):
    return i ^ k if n & (n - 1) == 0 else (i - k) % n


def split_of(size):
    inner = max(d for d in range(1, size + 1) if size % d == 0 and d * d <= size)
    return size // inner, inner


def size_of(v):
    return int(np.prod(v.shape)) * jnp.dtype(v.dtype).itemsize


def call(body, outs, *args, scratch=(), extra=0, local=False, flops=2000000, in_specs=None):
    held = sum(size_of(v) for v in args) + sum(size_of(v) for v in jax.tree.leaves(outs))
    held += sum(size_of(v) for v in scratch if hasattr(v, "dtype") and v.dtype in (F32, BF16))
    limit = min(60 * 1024 * 1024, held + extra + 6 * 1024 * 1024)
    in_specs = in_specs or [VMEM] * len(args)
    args = [
        pltpu.with_memory_space_constraint(v, pltpu.HBM)
        if spec is HBM
        else pltpu.with_memory_space_constraint(v, pltpu.VMEM)
        if spec is NEAR
        else v
        for v, spec in zip(args, in_specs)
    ]
    if local:
        outs = jax.tree.map(lambda v: pltpu.VMEM(v.shape, v.dtype), outs)
    return pl.pallas_call(
        body,
        out_shape=outs,
        in_specs=in_specs,
        out_specs=jax.tree.map(lambda _: VMEM, outs),
        scratch_shapes=list(scratch),
        compiler_params=pltpu.CompilerParams(vmem_limit_bytes=limit),
        cost_estimate=pl.CostEstimate(flops=flops, bytes_accessed=0, transcendentals=0),
    )(*args)


def sds(shape, dtype):
    return jax.ShapeDtypeStruct(shape, dtype)


def fetch_weights(sources, weight_ref, sems):
    moves, start = [], 0
    for i, source in enumerate(sources):
        columns = source.shape[1]
        moves.append(
            pltpu.make_async_copy(source, weight_ref.at[:, start : start + columns], sems.at[i])
        )
        moves[-1].start()
        start += columns
    return moves


def prepare_body(number, pad, ranks, outer, inner, *refs):
    here_ref, latent_hbm, context_hbm, weight_hbm = refs[:4]
    sources = refs[4:7]
    out_ref, table_ref, joined_ref, cond_ref, weight_ref, sems, more_sems = refs[7:]
    moves = [
        pltpu.make_async_copy(weight_hbm, weight_ref, sems.at[0]),
        pltpu.make_async_copy(latent_hbm, cond_ref.at[0:1], sems.at[1]),
        pltpu.make_async_copy(context_hbm, cond_ref.at[1:2], sems.at[2]),
    ]
    for move in moves:
        move.start()
    more = fetch_weights(sources, joined_ref, more_sems)
    make_tables(number, pad, ranks, outer, inner, here_ref[0], table_ref)
    moves[1].wait()
    moves[2].wait()
    rows = cond_ref[...]
    rows = (rows / (1.0 + jnp.exp(-rows))).astype(BF16)
    moves[0].wait()
    part = jnp.dot(rows, weight_ref[...], preferred_element_type=F32).astype(BF16)
    for i in range(out_ref.shape[0]):
        out_ref[i] = part
    for move in more:
        move.wait()


def make_tables(number, pad, ranks, outer, inner, here, out_ref):
    group, rank = lax.div(here, ranks), lax.rem(here, ranks)
    here_outer, here_inner = lax.div(rank, inner), lax.rem(rank, inner)
    lane = lax.broadcasted_iota(jnp.int32, (pad, 2 * QK_DIM), 1)
    line = lax.broadcasted_iota(jnp.int32, (pad, 2 * QK_DIM), 0)
    low = lane < QK_DIM
    by_row = (lane & (QK_DIM - 1)) < QK_DIM // 2
    sign = jnp.where((lane & (QK_DIM // 4)) == 0, -1.0, 1.0)
    phase = jnp.where(low, np.float32(np.pi / 2), np.float32(0))
    shift = GRID_W.bit_length() - 1
    quarter = QK_DIM // 4
    inverse = jnp.ones(lane.shape, F32)
    for i in range(1, quarter):
        inverse = jnp.where((lane & (quarter - 1)) == i, np.float32(THETA ** (-i / quarter)), inverse)

    def owner(i, k, n):
        return i ^ k if n & (n - 1) == 0 else lax.rem(i + (n - k), n)

    for j in range(inner):
        for k in range(outer):
            rank_at = owner(here_outer, k, outer) * inner + owner(here_inner, j, inner)
            position = line + (group * ranks + rank_at) * number
            place = jnp.where(by_row, position >> shift, position & (GRID_W - 1)).astype(F32)
            wave = jnp.sin(place * inverse + phase)
            other = pltpu.roll(wave, QK_DIM, 1)
            out_ref[j, 0, k * pad : (k + 1) * pad, :] = jnp.where(low, wave, other)
            out_ref[j, 1, k * pad : (k + 1) * pad, :] = jnp.where(low, other, wave) * sign


def modulated(values, shift, scale):
    values = values.astype(F32)
    mean = jnp.mean(values * values, axis=-1, keepdims=True)
    return (values * lax.rsqrt(mean + NORM_EPS) * scale + shift).astype(BF16)


def fill_rows(blocks, rows_ref, pad, shift, scale):
    number = blocks[0].shape[0]
    for k, block in enumerate(blocks):
        rows_ref[k * pad : k * pad + number, :] = modulated(block[...], shift, scale)
        if pad > number:
            rows_ref[k * pad + number : (k + 1) * pad, :] = jnp.zeros(
                (pad - number, rows_ref.shape[1]), BF16
            )


def turn(u, cosine, sine):
    lane = lax.broadcasted_iota(jnp.int32, u.shape, 1)
    quarter = QK_DIM // 4
    width = u.shape[1]
    even = (lane // quarter) % 2 == 0
    turned = jnp.where(even, pltpu.roll(u, width - quarter, 1), pltpu.roll(u, quarter, 1))
    return (u * cosine + turned * sine).astype(BF16)


def context_body(ranks, *refs):
    pieces_ref, context_hbm, weight_ref, mod_ref, kv_ref, context_ref, sem = refs
    move = pltpu.make_async_copy(context_hbm, context_ref, sem)
    move.start()
    held, width = context_ref.shape
    columns = pieces_ref.shape[2]
    groups = pieces_ref.shape[0] // ranks
    for t in range(ranks):
        total = pieces_ref[t].astype(F32)
        for s in range(1, groups):
            total = total + pieces_ref[s * ranks + t].astype(F32)
        mod_ref[:, t * columns : (t + 1) * columns] = total
    shift, scale = mod_ref[1:2, :width], 1.0 + mod_ref[1:2, width : 2 * width]
    step = 16 if held % 16 == 0 else held
    move.wait()
    for i in range(0, held, step):
        context_ref[i : i + step, :] = modulated(context_ref[i : i + step, :], shift, scale)
    kv_ref[...] = jnp.dot(
        context_ref[...], weight_ref[:, 2 * QK_DIM :], preferred_element_type=F32
    ).astype(BF16)


def rows_body(pad, outer, inner, *refs):
    mod_ref, table_ref, weight_ref = refs[:3]
    blocks = refs[3:-3]
    q_ref, kv_ref, rows_ref = refs[-3:]
    width = blocks[0].shape[1]
    fill_rows(
        blocks, rows_ref, pad, mod_ref[0:1, :width], 1.0 + mod_ref[0:1, width : 2 * width]
    )
    tile, wide = outer * pad, 2 * QK_DIM
    product = jnp.dot(rows_ref[...], weight_ref[...], preferred_element_type=F32)
    for j in range(inner):
        u = product[j * tile : (j + 1) * tile]
        cosine, sine = table_ref[j, 0], table_ref[j, 1]
        scale = jnp.asarray(QK_DIM ** (-0.5), BF16)
        q_ref[j] = turn(u[:, :wide], cosine, sine) * scale
        kv_ref[j * tile : (j + 1) * tile, :wide] = turn(u[:, wide : 2 * wide], cosine, sine)
        kv_ref[j * tile : (j + 1) * tile, wide:] = u[:, 2 * wide :].astype(BF16)


def gather_pieces(pieces, padded, number, pad, k_all, v_all):
    wide = 2 * QK_DIM
    row = latents = 0
    for i, piece in enumerate(pieces):
        rows = piece.shape[0]
        k_all[row : row + rows, :] = piece[:, :wide]
        v_all[row : row + rows, :] = piece[:, wide:]
        row += rows
        latents += rows if i < padded else 0
    column = lax.broadcasted_iota(jnp.int32, (1, row), 1)
    valid = (column >= latents) | (column % pad < number)
    return jnp.where(valid, 0.0, -1e30)


def score(q_ref, j, m, k_all):
    queries = q_ref[j]
    lane = lax.broadcasted_iota(jnp.int32, queries.shape, 1)
    own = jnp.where((lane // QK_DIM) == m, queries, jnp.zeros_like(queries))
    return lax.dot_general(
        own, k_all[...], (((1,), (1,)), ((), ())), preferred_element_type=F32
    )


def repeat(count, one):
    if count <= 4:
        for j in range(count):
            one(j, 0)
    else:
        lax.fori_loop(0, count, one, 0)


def attend_first_body(number, pad, padded, inner, *refs):
    q_ref, kv_refs = refs[0], refs[1:-5]
    top_ref, sum_ref, mix_ref, k_all, v_all = refs[-5:]
    bias = gather_pieces(kv_refs, padded, number, pad, k_all, v_all)

    def one(j, carry):
        for m in range(2):
            scores = score(q_ref, j, m, k_all) + bias
            highest = jnp.max(scores, axis=-1, keepdims=True)
            weights = jnp.exp(scores - highest)
            top_ref[j, m] = highest
            sum_ref[j, m] = jnp.sum(weights, axis=-1, keepdims=True)
            mix_ref[j, m] = jnp.dot(
                weights.astype(BF16), v_all[...], preferred_element_type=F32
            )
        return carry

    repeat(inner, one)


def attend_last_body(number, pad, outer, inner, *refs):
    factor_ref, top_ref, sum_ref, mix_ref, q_ref = refs[:5]
    kv_refs, (out_ref, k_all, v_all) = refs[5:-3], refs[-3:]
    bias = gather_pieces(kv_refs, len(kv_refs), number, pad, k_all, v_all)

    def one(j, carry):
        mixed = []
        for m in range(2):
            scores = score(q_ref, j, m, k_all) + bias
            before = top_ref[j, m]
            highest = jnp.maximum(before, jnp.max(scores, axis=-1, keepdims=True))
            fade = jnp.exp(before - highest)
            weights = jnp.exp(scores - highest)
            totals = sum_ref[j, m] * fade + jnp.sum(weights, axis=-1, keepdims=True)
            mix = mix_ref[j, m] * fade + jnp.dot(
                weights.astype(BF16), v_all[...], preferred_element_type=F32
            )
            mixed.append(mix / totals)
        head = mixed[0] - factor_ref[0] * mixed[1]
        head = head * lax.rsqrt(jnp.mean(head * head, axis=-1, keepdims=True) + HEAD_EPS)
        head = head.astype(BF16)
        for k in range(outer):
            out_ref[k, j] = head[k * pad : (k + 1) * pad]
        return carry

    repeat(inner, one)


def partial_out_body(slots, share, ranks, outer, inner, pad, *refs):
    here_ref, own_weight = refs[:2]
    held = refs[2 : 2 + len(slots)]
    rest = refs[2 + len(slots) :]
    parts, own_ref, others = rest[:outer], rest[outer], rest[1 + outer :]
    rows = inner * pad
    side = lax.rem(lax.div(here_ref[0], ranks), share)
    first = jnp.broadcast_to(side, (rows, VAL_DIM)) == 0

    def part(k):
        return parts[k][...].reshape(rows, VAL_DIM)

    total, start = None, 0
    for (a, b), weight in zip(slots, held):
        rows_in = part(a) if a == b else jnp.where(first, part(a), part(b))
        rows_in = rows_in[:, start : start + weight.shape[0]]
        start = (start + weight.shape[0]) % VAL_DIM
        term = jnp.dot(rows_in, weight[...], preferred_element_type=F32)
        total = term if total is None else total + term
    total += jnp.dot(part(0), own_weight[...], preferred_element_type=F32)
    own_ref[...] = total[:pad]
    for j in range(1, inner):
        others[j - 1][...] = total[j * pad : (j + 1) * pad].astype(BF16)


def final_body(count, *refs):
    latent_ref, mod_ref, own_ref = refs[:3]
    others = refs[3 : 3 + count]
    out_ref = refs[3 + count]
    number, width = out_ref.shape
    total = own_ref[...]
    for other in others:
        total = total + other[...].astype(F32)
    total = total[:number]
    total = total * lax.rsqrt(jnp.mean(total * total, axis=-1, keepdims=True) + NORM_EPS)
    gate = mod_ref[0:1, 2 * width :]
    out_ref[...] = (latent_ref[...].astype(F32) + gate * total).astype(BF16)


def shards(
    latent,
    context,
    cond_latent,
    cond_context,
    mod_weight,
    w_query,
    w_key,
    w_value,
    w_out,
    head_lambda,
):
    number, width = latent.shape
    groups, ranks = lax.axis_size("sp"), lax.axis_size("tp")
    outer, inner = split_of(ranks)
    pad = -(-number // 16) * 16
    wide = 2 * QK_DIM
    tile = outer * pad
    held = context.shape[0]
    here_sp, here_tp = lax.axis_index("sp"), lax.axis_index("tp")

    def along_outer(value, k, way):
        pairs = [
            (o * inner + i, way(o, k, outer) * inner + i)
            for o in range(outer)
            for i in range(inner)
        ]
        return lax.ppermute(value, "tp", pairs)

    def along_inner(value, j, way):
        pairs = [
            (o * inner + i, o * inner + way(i, j, inner))
            for o in range(outer)
            for i in range(inner)
        ]
        return lax.ppermute(value, "tp", pairs)

    columns = mod_weight.shape[1]
    here = (here_sp * ranks + here_tp).astype(jnp.int32).reshape(1)
    copies, table, weight = call(
        functools.partial(prepare_body, number, pad, ranks, outer, inner),
        (
            sds((groups * ranks, 2, columns), BF16),
            sds((inner, 2, tile, wide), F32),
            sds((width, wide + wide + VAL_DIM), BF16),
        ),
        here,
        cond_latent.reshape(1, -1),
        cond_context.reshape(1, -1),
        mod_weight,
        w_query,
        w_key,
        w_value,
        scratch=[
            pltpu.VMEM((2, cond_latent.shape[0]), F32),
            pltpu.VMEM(mod_weight.shape, BF16),
            pltpu.SemaphoreType.DMA((3,)),
            pltpu.SemaphoreType.DMA((3,)),
        ],
        in_specs=[SMEM] + [HBM] * 6,
        local=True,
    )
    pieces = lax.all_to_all(copies, ("sp", "tp"), 0, 0)

    blocks = {(0, 0): latent}
    for k in range(1, outer):
        if relayed(k):
            blocks[k, 0] = along_outer(blocks[k - 1, 0], 1, ahead)
        else:
            blocks[k, 0] = along_outer(latent, k, ahead)
    for j in range(1, inner):
        for k in range(outer):
            blocks[k, j] = along_inner(blocks[k, 0], j, ahead)

    mod, kv_context = call(
        functools.partial(context_body, ranks),
        (sds((2, columns * ranks), F32), sds((held, wide + VAL_DIM), BF16)),
        pieces,
        context,
        weight,
        scratch=[pltpu.VMEM((held, width), BF16), pltpu.SemaphoreType.DMA],
        in_specs=[VMEM, HBM, VMEM],
        local=True,
    )
    queries, kv = call(
        functools.partial(rows_body, pad, outer, inner),
        (sds((inner, tile, wide), BF16), sds((inner * tile, wide + VAL_DIM), BF16)),
        mod,
        table,
        weight,
        *[blocks[k, j] for j in range(inner) for k in range(outer)],
        scratch=[pltpu.VMEM((inner * tile, width), BF16)],
        extra=inner * tile * 6 * QK_DIM * 4,
        local=True,
    )
    share = share_of(groups)
    lines = groups // share

    def along_lines(value, s):
        pairs = [
            (g * share + c, ahead(g, s, lines) * share + c)
            for g in range(lines)
            for c in range(share)
        ]
        return lax.ppermute(value, "sp", pairs)

    swap = [(i, i ^ 1) for i in range(groups)]

    def spread(part):
        pieces = [part]
        for s in range(1, lines):
            pieces.append(along_lines(part, s))
        if share > 1:
            for piece in list(pieces):
                pieces.append(lax.ppermute(piece, "sp", swap))
        return pieces

    near, late = spread(kv_context), spread(kv)
    first = [i for i in range(len(late)) if i % lines == 0]
    early = [late[i] for i in first] + near
    late = [v for i, v in enumerate(late) if i not in first]
    stats = (
        sds((inner, 2, tile, 1), F32),
        sds((inner, 2, tile, 1), F32),
        sds((inner, 2, tile, VAL_DIM), F32),
    )

    def room(keys):
        return [pltpu.VMEM((keys, wide), BF16), pltpu.VMEM((keys, VAL_DIM), BF16)]

    keys = groups * held + len(first) * inner * tile
    first_stats = call(
        functools.partial(attend_first_body, number, pad, len(first), inner),
        stats,
        queries,
        *early,
        scratch=room(keys),
        extra=tile * keys * 12,
        local=True,
    )
    keys = len(late) * inner * tile
    attended = call(
        functools.partial(attend_last_body, number, pad, outer, inner),
        sds((outer, inner, pad, VAL_DIM), BF16),
        head_lambda,
        *first_stats,
        queries,
        *late,
        scratch=room(keys),
        extra=tile * keys * 12,
        in_specs=[SMEM] + [VMEM] * (4 + len(late)),
        local=True,
    )
    parts = [attended[0]]
    for k in range(1, outer):
        parts.append(along_outer(attended[k], k, behind))

    def joint(value, target):
        moves = []
        for s in range(groups):
            for o in range(outer):
                for i in range(inner):
                    to_s, to_o = target(s, o)
                    moves.append(
                        ((s * outer + o) * inner + i, (to_s * outer + to_o) * inner + i)
                    )
        return lax.ppermute(value, ("sp", "tp"), moves)

    slots, weights = [], []
    if share > 1 and outer == 4:
        fetched = joint(w_out, lambda s, o: (s, behind(o, 1 if s % 2 else 2, outer)))
        turned = joint(fetched, lambda s, o: (s ^ 1, o if s % 2 else behind(o, 1, outer)))
        given = jnp.where(here_sp % 2 == 0, fetched, turned)
        traded = lax.ppermute(given, "sp", swap)
        slots, weights = [(2, 1), (1, 3), (3, 2)], [fetched, turned, traded]
    else:
        for k in range(1, outer):
            weights.append(along_outer(w_out, k, behind))
            slots.append((k, k))
    total = call(
        functools.partial(partial_out_body, slots, share, ranks, outer, inner, pad),
        (sds((pad, width), F32),) + (sds((pad, width), BF16),) * (inner - 1),
        here,
        w_out,
        *weights,
        *parts,
        in_specs=[SMEM] + [VMEM] * (1 + len(weights) + outer),
    )
    arrived = []
    for j in range(1, inner):
        arrived.append(along_inner(total[j], j, behind))
    return call(
        functools.partial(final_body, inner - 1),
        sds((number, width), BF16),
        latent,
        mod,
        total[0],
        *arrived,
    )


def relayed(k):
    return k > 1 and k % 2 == 1


def share_of(groups):
    return 2 if groups % 2 == 0 else 1


def solution(mesh):
    placed = (
        P(("sp", "tp"), None),
        P("sp", None),
        P("sp"),
        P("sp"),
        P("sp", "tp"),
        P(None, "tp"),
        P(None, "tp"),
        P(None, "tp"),
        P("tp", None),
        P("tp"),
    )
    return jax.shard_map(
        shards, mesh=mesh, in_specs=placed, out_specs=P(("sp", "tp"), None), check_vma=False
    )
```

```python
import functools

import jax
import jax.numpy as jnp
import numpy as np
from jax import lax
from jax.experimental import pallas as pl
from jax.experimental.pallas import tpu as pltpu
from jax.sharding import PartitionSpec as P

QK_DIM = 64
VAL_DIM = 128
GRID_W = 64

NORM_EPS = 0.01
HEAD_EPS = 0.001
THETA = 10000.0

F32 = jnp.float32
BF16 = jnp.bfloat16
VMEM = pl.BlockSpec(memory_space=pltpu.VMEM)
SMEM = pl.BlockSpec(memory_space=pltpu.SMEM)
NEAR = pl.BlockSpec(memory_space=pltpu.VMEM)
HBM = pl.BlockSpec(memory_space=pltpu.HBM)


def ahead(i, k, n):
    return i ^ k if n & (n - 1) == 0 else (i + k) % n


def behind(i, k, n):
    return i ^ k if n & (n - 1) == 0 else (i - k) % n


def split_of(size):
    inner = max(d for d in range(1, size + 1) if size % d == 0 and d * d <= size)
    return size // inner, inner


def size_of(v):
    return int(np.prod(v.shape)) * jnp.dtype(v.dtype).itemsize


def call(body, outs, *args, scratch=(), extra=0, local=False, flops=2000000, in_specs=None):
    held = sum(size_of(v) for v in args) + sum(size_of(v) for v in jax.tree.leaves(outs))
    held += sum(size_of(v) for v in scratch if hasattr(v, "dtype") and v.dtype in (F32, BF16))
    limit = min(60 * 1024 * 1024, held + extra + 6 * 1024 * 1024)
    in_specs = in_specs or [VMEM] * len(args)
    args = [
        pltpu.with_memory_space_constraint(v, pltpu.HBM)
        if spec is HBM
        else pltpu.with_memory_space_constraint(v, pltpu.VMEM)
        if spec is NEAR
        else v
        for v, spec in zip(args, in_specs)
    ]
    if local:
        outs = jax.tree.map(lambda v: pltpu.VMEM(v.shape, v.dtype), outs)
    return pl.pallas_call(
        body,
        out_shape=outs,
        in_specs=in_specs,
        out_specs=jax.tree.map(lambda _: VMEM, outs),
        scratch_shapes=list(scratch),
        compiler_params=pltpu.CompilerParams(vmem_limit_bytes=limit),
        cost_estimate=pl.CostEstimate(flops=flops, bytes_accessed=0, transcendentals=0),
    )(*args)


def sds(shape, dtype):
    return jax.ShapeDtypeStruct(shape, dtype)


def fetch_weights(sources, weight_ref, sems):
    moves, start = [], 0
    for i, source in enumerate(sources):
        columns = source.shape[1]
        moves.append(
            pltpu.make_async_copy(source, weight_ref.at[:, start : start + columns], sems.at[i])
        )
        moves[-1].start()
        start += columns
    return moves


def prepare_body(number, pad, ranks, outer, inner, *refs):
    here_ref, latent_hbm, context_hbm, weight_hbm = refs[:4]
    sources = refs[4:7]
    out_ref, table_ref, joined_ref, cond_ref, weight_ref, sems, more_sems = refs[7:]
    moves = [
        pltpu.make_async_copy(weight_hbm, weight_ref, sems.at[0]),
        pltpu.make_async_copy(latent_hbm, cond_ref.at[0:1], sems.at[1]),
        pltpu.make_async_copy(context_hbm, cond_ref.at[1:2], sems.at[2]),
    ]
    for move in moves:
        move.start()
    more = fetch_weights(sources, joined_ref, more_sems)
    make_tables(number, pad, ranks, outer, inner, here_ref[0], table_ref)
    moves[1].wait()
    moves[2].wait()
    rows = cond_ref[...]
    rows = (rows / (1.0 + jnp.exp(-rows))).astype(BF16)
    moves[0].wait()
    part = jnp.dot(rows, weight_ref[...], preferred_element_type=F32).astype(BF16)
    for i in range(out_ref.shape[0]):
        out_ref[i] = part
    for move in more:
        move.wait()


def make_tables(number, pad, ranks, outer, inner, here, out_ref):
    group, rank = lax.div(here, ranks), lax.rem(here, ranks)
    here_outer, here_inner = lax.div(rank, inner), lax.rem(rank, inner)
    lane = lax.broadcasted_iota(jnp.int32, (pad, 2 * QK_DIM), 1)
    line = lax.broadcasted_iota(jnp.int32, (pad, 2 * QK_DIM), 0)
    low = lane < QK_DIM
    by_row = (lane & (QK_DIM - 1)) < QK_DIM // 2
    sign = jnp.where((lane & (QK_DIM // 4)) == 0, -1.0, 1.0)
    phase = jnp.where(low, np.float32(np.pi / 2), np.float32(0))
    shift = GRID_W.bit_length() - 1
    quarter = QK_DIM // 4
    inverse = jnp.ones(lane.shape, F32)
    for i in range(1, quarter):
        inverse = jnp.where((lane & (quarter - 1)) == i, np.float32(THETA ** (-i / quarter)), inverse)

    def owner(i, k, n):
        return i ^ k if n & (n - 1) == 0 else lax.rem(i + (n - k), n)

    for j in range(inner):
        for k in range(outer):
            rank_at = owner(here_outer, k, outer) * inner + owner(here_inner, j, inner)
            position = line + (group * ranks + rank_at) * number
            place = jnp.where(by_row, position >> shift, position & (GRID_W - 1)).astype(F32)
            wave = jnp.sin(place * inverse + phase)
            other = pltpu.roll(wave, QK_DIM, 1)
            out_ref[j, 0, k * pad : (k + 1) * pad, :] = jnp.where(low, wave, other)
            out_ref[j, 1, k * pad : (k + 1) * pad, :] = jnp.where(low, other, wave) * sign


def modulated(values, shift, scale):
    values = values.astype(F32)
    mean = jnp.mean(values * values, axis=-1, keepdims=True)
    return (values * lax.rsqrt(mean + NORM_EPS) * scale + shift).astype(BF16)


def fill_rows(blocks, rows_ref, pad, shift, scale):
    number = blocks[0].shape[0]
    for k, block in enumerate(blocks):
        rows_ref[k * pad : k * pad + number, :] = modulated(block[...], shift, scale)
        if pad > number:
            rows_ref[k * pad + number : (k + 1) * pad, :] = jnp.zeros(
                (pad - number, rows_ref.shape[1]), BF16
            )


def turn(u, cosine, sine):
    lane = lax.broadcasted_iota(jnp.int32, u.shape, 1)
    quarter = QK_DIM // 4
    width = u.shape[1]
    even = (lane // quarter) % 2 == 0
    turned = jnp.where(even, pltpu.roll(u, width - quarter, 1), pltpu.roll(u, quarter, 1))
    return (u * cosine + turned * sine).astype(BF16)


def context_body(ranks, *refs):
    pieces_ref, context_hbm, weight_ref, mod_ref, kv_ref, context_ref, sem = refs
    move = pltpu.make_async_copy(context_hbm, context_ref, sem)
    move.start()
    held, width = context_ref.shape
    columns = pieces_ref.shape[2]
    groups = pieces_ref.shape[0] // ranks
    for t in range(ranks):
        total = pieces_ref[t].astype(F32)
        for s in range(1, groups):
            total = total + pieces_ref[s * ranks + t].astype(F32)
        mod_ref[:, t * columns : (t + 1) * columns] = total
    shift, scale = mod_ref[1:2, :width], 1.0 + mod_ref[1:2, width : 2 * width]
    step = 16 if held % 16 == 0 else held
    move.wait()
    for i in range(0, held, step):
        context_ref[i : i + step, :] = modulated(context_ref[i : i + step, :], shift, scale)
    kv_ref[...] = jnp.dot(
        context_ref[...], weight_ref[:, 2 * QK_DIM :], preferred_element_type=F32
    ).astype(BF16)


def rows_body(pad, outer, inner, *refs):
    mod_ref, table_ref, weight_ref = refs[:3]
    blocks = refs[3:-3]
    q_ref, kv_ref, rows_ref = refs[-3:]
    width = blocks[0].shape[1]
    fill_rows(
        blocks, rows_ref, pad, mod_ref[0:1, :width], 1.0 + mod_ref[0:1, width : 2 * width]
    )
    tile, wide = outer * pad, 2 * QK_DIM
    product = jnp.dot(rows_ref[...], weight_ref[...], preferred_element_type=F32)
    for j in range(inner):
        u = product[j * tile : (j + 1) * tile]
        cosine, sine = table_ref[j, 0], table_ref[j, 1]
        scale = jnp.asarray(QK_DIM ** (-0.5), BF16)
        q_ref[j] = turn(u[:, :wide], cosine, sine) * scale
        kv_ref[j * tile : (j + 1) * tile, :wide] = turn(u[:, wide : 2 * wide], cosine, sine)
        kv_ref[j * tile : (j + 1) * tile, wide:] = u[:, 2 * wide :].astype(BF16)


def gather_pieces(pieces, padded, number, pad, k_all, v_all):
    wide = 2 * QK_DIM
    row = latents = 0
    for i, piece in enumerate(pieces):
        rows = piece.shape[0]
        k_all[row : row + rows, :] = piece[:, :wide]
        v_all[row : row + rows, :] = piece[:, wide:]
        row += rows
        latents += rows if i < padded else 0
    column = lax.broadcasted_iota(jnp.int32, (1, row), 1)
    valid = (column >= latents) | (column % pad < number)
    return jnp.where(valid, 0.0, -1e30)


def score(q_ref, j, m, k_all):
    queries = q_ref[j]
    lane = lax.broadcasted_iota(jnp.int32, queries.shape, 1)
    own = jnp.where((lane // QK_DIM) == m, queries, jnp.zeros_like(queries))
    return lax.dot_general(
        own, k_all[...], (((1,), (1,)), ((), ())), preferred_element_type=F32
    )


def repeat(count, one):
    if count <= 4:
        for j in range(count):
            one(j, 0)
    else:
        lax.fori_loop(0, count, one, 0)


def attend_first_body(number, pad, padded, inner, *refs):
    exit_hbm, q_ref, kv_refs = refs[0], refs[1], refs[2:-7]
    top_ref, sum_ref, mix_ref, exit_ref, k_all, v_all, sem = refs[-7:]
    move = pltpu.make_async_copy(exit_hbm, exit_ref, sem)
    move.start()
    bias = gather_pieces(kv_refs, padded, number, pad, k_all, v_all)

    def one(j, carry):
        for m in range(2):
            scores = score(q_ref, j, m, k_all) + bias
            highest = jnp.max(scores, axis=-1, keepdims=True)
            weights = jnp.exp(scores - highest)
            top_ref[j, m] = highest
            sum_ref[j, m] = jnp.sum(weights, axis=-1, keepdims=True)
            mix_ref[j, m] = jnp.dot(
                weights.astype(BF16), v_all[...], preferred_element_type=F32
            )
        return carry

    repeat(inner, one)
    move.wait()


def attend_last_body(number, pad, outer, inner, *refs):
    factor_ref, top_ref, sum_ref, mix_ref, q_ref = refs[:5]
    kv_refs, (out_ref, k_all, v_all) = refs[5:-3], refs[-3:]
    bias = gather_pieces(kv_refs, len(kv_refs), number, pad, k_all, v_all)

    def one(j, carry):
        mixed = []
        for m in range(2):
            scores = score(q_ref, j, m, k_all) + bias
            before = top_ref[j, m]
            highest = jnp.maximum(before, jnp.max(scores, axis=-1, keepdims=True))
            fade = jnp.exp(before - highest)
            weights = jnp.exp(scores - highest)
            totals = sum_ref[j, m] * fade + jnp.sum(weights, axis=-1, keepdims=True)
            mix = mix_ref[j, m] * fade + jnp.dot(
                weights.astype(BF16), v_all[...], preferred_element_type=F32
            )
            mixed.append(mix / totals)
        head = mixed[0] - factor_ref[0] * mixed[1]
        head = head * lax.rsqrt(jnp.mean(head * head, axis=-1, keepdims=True) + HEAD_EPS)
        head = head.astype(BF16)
        for k in range(outer):
            out_ref[k, j] = head[k * pad : (k + 1) * pad]
        return carry

    repeat(inner, one)


def partial_out_body(slots, share, ranks, outer, inner, pad, *refs):
    here_ref, own_weight = refs[:2]
    held = refs[2 : 2 + len(slots)]
    rest = refs[2 + len(slots) :]
    parts, own_ref, others = rest[:outer], rest[outer], rest[1 + outer :]
    rows = inner * pad
    side = lax.rem(lax.div(here_ref[0], ranks), share)
    first = jnp.broadcast_to(side, (rows, VAL_DIM)) == 0

    def part(k):
        return parts[k][...].reshape(rows, VAL_DIM)

    total, start = None, 0
    for (a, b), weight in zip(slots, held):
        rows_in = part(a) if a == b else jnp.where(first, part(a), part(b))
        rows_in = rows_in[:, start : start + weight.shape[0]]
        start = (start + weight.shape[0]) % VAL_DIM
        term = jnp.dot(rows_in, weight[...], preferred_element_type=F32)
        total = term if total is None else total + term
    total += jnp.dot(part(0), own_weight[...], preferred_element_type=F32)
    own_ref[...] = total[:pad]
    for j in range(1, inner):
        others[j - 1][...] = total[j * pad : (j + 1) * pad].astype(BF16)


def final_body(count, *refs):
    latent_ref, mod_ref, own_ref = refs[:3]
    others = refs[3 : 3 + count]
    out_ref = refs[3 + count]
    number, width = out_ref.shape
    total = own_ref[...]
    for other in others:
        total = total + other[...].astype(F32)
    total = total[:number]
    total = total * lax.rsqrt(jnp.mean(total * total, axis=-1, keepdims=True) + NORM_EPS)
    gate = mod_ref[0:1, 2 * width :]
    out_ref[...] = (latent_ref[...].astype(F32) + gate * total).astype(BF16)


def shards(
    latent,
    context,
    cond_latent,
    cond_context,
    mod_weight,
    w_query,
    w_key,
    w_value,
    w_out,
    head_lambda,
):
    number, width = latent.shape
    groups, ranks = lax.axis_size("sp"), lax.axis_size("tp")
    outer, inner = split_of(ranks)
    pad = -(-number // 16) * 16
    wide = 2 * QK_DIM
    tile = outer * pad
    held = context.shape[0]
    here_sp, here_tp = lax.axis_index("sp"), lax.axis_index("tp")

    def along_outer(value, k, way):
        pairs = [
            (o * inner + i, way(o, k, outer) * inner + i)
            for o in range(outer)
            for i in range(inner)
        ]
        return lax.ppermute(value, "tp", pairs)

    def along_inner(value, j, way):
        pairs = [
            (o * inner + i, o * inner + way(i, j, inner))
            for o in range(outer)
            for i in range(inner)
        ]
        return lax.ppermute(value, "tp", pairs)

    columns = mod_weight.shape[1]
    here = (here_sp * ranks + here_tp).astype(jnp.int32).reshape(1)
    copies, table, weight = call(
        functools.partial(prepare_body, number, pad, ranks, outer, inner),
        (
            sds((groups * ranks, 2, columns), BF16),
            sds((inner, 2, tile, wide), F32),
            sds((width, wide + wide + VAL_DIM), BF16),
        ),
        here,
        cond_latent.reshape(1, -1),
        cond_context.reshape(1, -1),
        mod_weight,
        w_query,
        w_key,
        w_value,
        scratch=[
            pltpu.VMEM((2, cond_latent.shape[0]), F32),
            pltpu.VMEM(mod_weight.shape, BF16),
            pltpu.SemaphoreType.DMA((3,)),
            pltpu.SemaphoreType.DMA((3,)),
        ],
        in_specs=[SMEM] + [HBM] * 6,
        local=True,
    )
    pieces = lax.all_to_all(copies, ("sp", "tp"), 0, 0)

    blocks = {(0, 0): latent}
    for k in range(1, outer):
        if relayed(k):
            blocks[k, 0] = along_outer(blocks[k - 1, 0], 1, ahead)
        else:
            blocks[k, 0] = along_outer(latent, k, ahead)
    for j in range(1, inner):
        for k in range(outer):
            blocks[k, j] = along_inner(blocks[k, 0], j, ahead)

    mod, kv_context = call(
        functools.partial(context_body, ranks),
        (sds((2, columns * ranks), F32), sds((held, wide + VAL_DIM), BF16)),
        pieces,
        context,
        weight,
        scratch=[pltpu.VMEM((held, width), BF16), pltpu.SemaphoreType.DMA],
        in_specs=[VMEM, HBM, VMEM],
        local=True,
    )
    queries, kv = call(
        functools.partial(rows_body, pad, outer, inner),
        (sds((inner, tile, wide), BF16), sds((inner * tile, wide + VAL_DIM), BF16)),
        mod,
        table,
        weight,
        *[blocks[k, j] for j in range(inner) for k in range(outer)],
        scratch=[pltpu.VMEM((inner * tile, width), BF16)],
        extra=inner * tile * 6 * QK_DIM * 4,
        local=True,
    )
    share = share_of(groups)
    lines = groups // share

    def along_lines(value, s):
        pairs = [
            (g * share + c, ahead(g, s, lines) * share + c)
            for g in range(lines)
            for c in range(share)
        ]
        return lax.ppermute(value, "sp", pairs)

    swap = [(i, i ^ 1) for i in range(groups)]

    def spread(part):
        pieces = [part]
        for s in range(1, lines):
            pieces.append(along_lines(part, s))
        if share > 1:
            for piece in list(pieces):
                pieces.append(lax.ppermute(piece, "sp", swap))
        return pieces

    near, late = spread(kv_context), spread(kv)
    first = [i for i in range(len(late)) if i % lines == 0]
    early = [late[i] for i in first] + near
    late = [v for i, v in enumerate(late) if i not in first]
    stats = (
        sds((inner, 2, tile, 1), F32),
        sds((inner, 2, tile, 1), F32),
        sds((inner, 2, tile, VAL_DIM), F32),
    )

    def room(keys):
        return [pltpu.VMEM((keys, wide), BF16), pltpu.VMEM((keys, VAL_DIM), BF16)]

    keys = groups * held + len(first) * inner * tile
    *first_stats, exit_weight = call(
        functools.partial(attend_first_body, number, pad, len(first), inner),
        stats + (sds(w_out.shape, BF16),),
        w_out,
        queries,
        *early,
        scratch=room(keys) + [pltpu.SemaphoreType.DMA],
        extra=tile * keys * 12,
        in_specs=[HBM] + [VMEM] * (1 + len(early)),
        local=True,
    )
    keys = len(late) * inner * tile
    attended = call(
        functools.partial(attend_last_body, number, pad, outer, inner),
        sds((outer, inner, pad, VAL_DIM), BF16),
        head_lambda,
        *first_stats,
        queries,
        *late,
        scratch=room(keys),
        extra=tile * keys * 12,
        in_specs=[SMEM] + [VMEM] * (4 + len(late)),
        local=True,
    )
    parts = [attended[0]]
    for k in range(1, outer):
        parts.append(along_outer(attended[k], k, behind))

    def joint(value, target):
        moves = []
        for s in range(groups):
            for o in range(outer):
                for i in range(inner):
                    to_s, to_o = target(s, o)
                    moves.append(
                        ((s * outer + o) * inner + i, (to_s * outer + to_o) * inner + i)
                    )
        return lax.ppermute(value, ("sp", "tp"), moves)

    slots, weights = [], []
    if share > 1 and outer == 4:
        fetched = joint(w_out, lambda s, o: (s, behind(o, 1 if s % 2 else 2, outer)))
        turned = joint(fetched, lambda s, o: (s ^ 1, o if s % 2 else behind(o, 1, outer)))
        given = jnp.where(here_sp % 2 == 0, fetched, turned)
        traded = lax.ppermute(given, "sp", swap)
        slots, weights = [(2, 1), (1, 3), (3, 2)], [fetched, turned, traded]
    else:
        for k in range(1, outer):
            weights.append(along_outer(w_out, k, behind))
            slots.append((k, k))
    total = call(
        functools.partial(partial_out_body, slots, share, ranks, outer, inner, pad),
        (sds((pad, width), F32),) + (sds((pad, width), BF16),) * (inner - 1),
        here,
        exit_weight,
        *weights,
        *parts,
        in_specs=[SMEM] + [VMEM] * (1 + len(weights) + outer),
    )
    arrived = []
    for j in range(1, inner):
        arrived.append(along_inner(total[j], j, behind))
    return call(
        functools.partial(final_body, inner - 1),
        sds((number, width), BF16),
        latent,
        mod,
        total[0],
        *arrived,
    )


def relayed(k):
    return k > 1 and k % 2 == 1


def share_of(groups):
    return 2 if groups % 2 == 0 else 1


def solution(mesh):
    placed = (
        P(("sp", "tp"), None),
        P("sp", None),
        P("sp"),
        P("sp"),
        P("sp", "tp"),
        P(None, "tp"),
        P(None, "tp"),
        P(None, "tp"),
        P("tp", None),
        P("tp"),
    )
    return jax.shard_map(
        shards, mesh=mesh, in_specs=placed, out_specs=P(("sp", "tp"), None), check_vma=False
    )
```
